512 devices in a mesh: sp: 16 (over z), fs: 4 (over y), tp: 8 (over x, core).
Axes of the slice: x: 4, y: 4, z: 16, core: 2. Of those that a mesh axis runs over, the one named last changes fastest.
Arguments:
- inputs: bfloat16 [4, 8192, 2048], P('fs', 'sp', 'tp'), may hold values from -6 to 6
- norm_gain: float32 [2048], replicated, may hold values from 0.1 to 1.9
- query_weight: bfloat16 [2048, 1024], P(('sp', 'fs'), 'tp'), may hold values from -0.125 to 0.125
- key_weight: bfloat16 [2048, 1024], P(('sp', 'fs'), 'tp'), may hold values from -0.125 to 0.125
- value_weight: bfloat16 [2048, 1024], P(('sp', 'fs'), 'tp'), may hold values from -0.125 to 0.125
- query_gain: float32 [64], replicated, may hold values from 0.8 to 7
- key_gain: float32 [64], replicated, may hold values from 0.8 to 7
- mix_lambda: float32 [8], replicated, may hold values from 0.3 to 0.8
- head_gain: float32 [128], replicated, may hold values from 0.1 to 1.9
- post_gate_weight: bfloat16 [2048, 2048], P(('sp', 'fs'), 'tp'), may hold values from -0.125 to 0.125
- pre_gate_weight: bfloat16 [2048, 2048], P(('sp', 'fs'), 'tp'), may hold values from -0.125 to 0.125
- inner_weight: bfloat16 [2048, 2048], P(('sp', 'fs'), 'tp'), may hold values from -0.125 to 0.125
- conv_taps: float32 [3, 2048], replicated, may hold values from -3 to 3
- attn_out_weight: bfloat16 [2048, 1024], P(('sp', 'fs'), 'tp'), may hold values from -0.109375 to 0.109375
- conv_out_weight: bfloat16 [2048, 2048], P(('sp', 'fs'), 'tp'), may hold values from -0.109375 to 0.109375
Outputs:
- mixed: bfloat16 [4, 8192, 2048], P('fs', ('sp', 'tp'))
The draws below stay inside these ranges and needn't reach their ends.
All inputs are finite; a program needn't handle non-finite values.
Results may differ from the reference program's by a relative error of at most 0.015.
The reference program's roundings to bfloat16 on the way count: a program that leaves them out, or rounds other values in their place, can miss the bound.
Values may be sent and summed in bfloat16 or wider, within the bound.
No kernel may reach another device: no remote copies, remote signals or barrier semaphores. Data moves between devices by JAX's collectives and lax.ppermute only.
A program may use at most 64 MiB of HBM per device.

```python
import math
import jax
import jax.numpy as jnp
from jax import lax

D = 2048
HEADS = 8
HALF = 64
VDIM = 128
LENGTH = 8192
SEQS = 4
N_TP = 8


def gain_draw(key, salt):
    lowest = 0.8
    highest = 1.8
    fraction = jax.random.uniform(jax.random.fold_in(key, salt), (HALF,), jnp.float32)
    return jnp.exp(jnp.log(lowest) + fraction * (jnp.log(highest) - jnp.log(lowest)))


def draw_query_gain(key, part):
    return gain_draw(key, 31)


def draw_key_gain(key, part):
    return gain_draw(key, 57)


def steps_of(own_key, shape, pieces, least, largest):
    level, own = 1.0, jax.random.fold_in(own_key, 6)
    for dim, parts in pieces:
        draws = jnp.exp(jax.random.uniform(jax.random.fold_in(own, dim), (parts,), jnp.float32, least / len(pieces), largest / len(pieces)))
        level = level * jnp.repeat(draws, shape[dim] // parts).reshape([-1 if axis == dim else 1 for axis in range(len(shape))])
    return level


def centred(rng, extent, scale, most, cuts=(), kind=jnp.bfloat16):
    values = jax.random.normal(rng, extent, jnp.float32) * scale
    if len(cuts) > 0:
        values = steps_of(rng, extent, cuts, -0.22, 0.18) * values
    return jnp.clip(values, min=-most, max=most).astype(kind)


def setup_inputs(seed: int = 0) -> dict:
    keys = jax.random.split(jax.random.key(seed), 16)
    return {
        "inputs": centred(keys[0], (SEQS, LENGTH, D), 1.0, 6.0, ((0, 4), (1, 16), (2, 8))),
        "norm_gain": jnp.clip(1.0 + 0.18 * jax.random.normal(keys[1], (D,), jnp.float32), 0.1, 1.9),
        "query_weight": centred(keys[2], (D, HEADS * 2 * HALF), D ** -0.5, 0.125, ((0, 64), (1, 8))),
        "key_weight": centred(keys[3], (D, HEADS * 2 * HALF), D ** -0.5, 0.125, ((0, 64), (1, 8))),
        "value_weight": centred(keys[4], (D, HEADS * VDIM), D ** -0.5, 0.125, ((0, 64), (1, 8))),
        "query_gain": draw_query_gain(jax.random.fold_in(keys[15], 71), 0),
        "key_gain": draw_key_gain(jax.random.fold_in(keys[15], 71), 0),
        "mix_lambda": jnp.clip(jax.random.uniform(keys[7], (HEADS,), jnp.float32, 0.3, 0.8), 0.3, 0.8),
        "head_gain": jnp.clip(1.0 + 0.18 * jax.random.normal(keys[8], (VDIM,), jnp.float32), 0.1, 1.9),
        "post_gate_weight": centred(keys[9], (D, D), D ** -0.5, 0.125, ((0, 64), (1, 8))),
        "pre_gate_weight": centred(keys[10], (D, D), D ** -0.5, 0.125, ((0, 64), (1, 8))),
        "inner_weight": centred(keys[11], (D, D), D ** -0.5, 0.125, ((0, 64), (1, 8))),
        "conv_taps": centred(keys[12], (3, D), 0.6, 3.0, (), jnp.float32),
        "attn_out_weight": centred(keys[13], (D, HEADS * VDIM), (HEADS * VDIM + D) ** -0.5, 0.109375, ((0, 64), (1, 8))),
        "conv_out_weight": centred(keys[14], (D, D), (HEADS * VDIM + D) ** -0.5, 0.109375, ((0, 64), (1, 8))),
    }


epsilon = 1e-06

def scale_rows(values, gain):
    return values * lax.rsqrt(lax.optimization_barrier(jnp.mean(values * values, axis=-1, keepdims=True)) + epsilon) * gain

def attend_head(query_head, key_head, value_head, weight_two):
    block = math.gcd(LENGTH, 512)
    query_blocks = jnp.transpose(query_head.reshape(2, LENGTH // block, block, HALF), (1, 0, 2, 3))
    keys_wide = key_head.astype(jnp.float32)
    values_wide = value_head.astype(jnp.float32)

    def one_block(query_block):
        scores = jnp.einsum('jqd,jkd->jqk', query_block.astype(jnp.float32), keys_wide) * HALF ** (-0.5)
        peak = lax.optimization_barrier(jnp.max(scores, axis=-1, keepdims=True))
        expo = jnp.exp(scores - peak)
        total = lax.optimization_barrier(jnp.sum(expo, axis=-1, keepdims=True))
        rounded = lax.optimization_barrier(expo.astype(jnp.bfloat16)).astype(jnp.float32)
        mapped = jnp.einsum('jqk,kd->jqd', rounded, values_wide) / total
        return mapped[0] - weight_two * mapped[1]
    result = lax.map(one_block, query_blocks)
    return result.reshape(LENGTH, VDIM)

def one_sequence(tokens, norm_gain, query_weight, key_weight, value_weight, query_gain, key_gain, mix_lambda, head_gain, post_gate_weight, pre_gate_weight, inner_weight, conv_taps, attn_out_weight, conv_out_weight):
    normed = scale_rows(tokens.astype(jnp.float32), norm_gain).astype(jnp.bfloat16)
    query = jnp.dot(normed, query_weight, preferred_element_type=jnp.float32).reshape(LENGTH, HEADS, 2, HALF)
    key = jnp.dot(normed, key_weight, preferred_element_type=jnp.float32).reshape(LENGTH, HEADS, 2, HALF)
    query_normed = scale_rows(query, query_gain).astype(jnp.bfloat16)
    key_normed = scale_rows(key, key_gain).astype(jnp.bfloat16)
    values = jnp.dot(normed, value_weight, preferred_element_type=jnp.float32).astype(jnp.bfloat16)
    values = values.reshape(LENGTH, HEADS, VDIM)

    def per_head(members):
        return attend_head(members[0], members[1], members[2], members[3])
    head_out = lax.map(per_head, (jnp.transpose(query_normed, (1, 2, 0, 3)), jnp.transpose(key_normed, (1, 2, 0, 3)), jnp.transpose(values, (1, 0, 2)), mix_lambda))
    attn_hidden = scale_rows(head_out, head_gain).astype(jnp.bfloat16)
    attn_hidden = jnp.transpose(attn_hidden, (1, 0, 2)).reshape(LENGTH, HEADS * VDIM)
    post = jnp.dot(normed, post_gate_weight, preferred_element_type=jnp.float32).astype(jnp.bfloat16)
    post_wide = lax.optimization_barrier(post).astype(jnp.float32)
    signal = (jnp.dot(normed, pre_gate_weight, preferred_element_type=jnp.float32) * jnp.dot(normed, inner_weight, preferred_element_type=jnp.float32)).astype(jnp.bfloat16)
    padded = jnp.pad(lax.optimization_barrier(signal).astype(jnp.float32), ((1, 1), (0, 0)))
    filtered = conv_taps[0] * padded[:-2] + conv_taps[1] * padded[1:-1] + conv_taps[2] * padded[2:]
    conv_hidden = (post_wide * filtered).astype(jnp.bfloat16)
    head_span = HEADS // N_TP * VDIM
    channel_span = D // N_TP
    summed = jnp.zeros((LENGTH, D), jnp.float32)
    for group in range(N_TP):
        attn_part = attn_hidden[:, group * head_span:(group + 1) * head_span]
        attn_cols = attn_out_weight[:, group * head_span:(group + 1) * head_span]
        conv_part = conv_hidden[:, group * channel_span:(group + 1) * channel_span]
        conv_cols = conv_out_weight[:, group * channel_span:(group + 1) * channel_span]
        partial_value = jnp.dot(attn_part, attn_cols.T, preferred_element_type=jnp.float32) + jnp.dot(conv_part, conv_cols.T, preferred_element_type=jnp.float32)
        summed = summed + lax.optimization_barrier(partial_value.astype(jnp.bfloat16)).astype(jnp.float32)
    return summed.astype(jnp.bfloat16)

def reference(inputs, norm_gain, query_weight, key_weight, value_weight, query_gain, key_gain, mix_lambda, head_gain, post_gate_weight, pre_gate_weight, inner_weight, conv_taps, attn_out_weight, conv_out_weight):
    results = []
    for sequence in range(SEQS):
        results.append(one_sequence(inputs[sequence], norm_gain, query_weight, key_weight, value_weight, query_gain, key_gain, mix_lambda, head_gain, post_gate_weight, pre_gate_weight, inner_weight, conv_taps, attn_out_weight, conv_out_weight))
    return jnp.stack(results, axis=0)
```

```python
import jax
import jax.numpy as jnp
from jax import lax
from jax.experimental import pallas as pl
from jax.experimental.pallas import tpu as pltpu
from jax.sharding import PartitionSpec as P

epsilon = 1e-06
log2e = 1.4426950408889634


def scale_rows(values, gain):
    return values * lax.rsqrt(jnp.mean(values * values, axis=-1, keepdims=True) + epsilon) * gain


def from_everyone(x, axis):
    copies = jnp.broadcast_to(x, (lax.axis_size(axis), *x.shape))
    return lax.all_to_all(copies, axis, split_axis=0, concat_axis=0, tiled=True)


def rows_in_order(tiles, sp, fs):
    rows, n = tiles.shape[1] // sp, tiles.shape[2]
    return jnp.transpose(tiles.reshape(fs, sp, rows, n), (1, 0, 2, 3)).reshape(fs * sp * rows, n)


def attention_kernel(q_ref, kv_ref, lam_ref, gain_ref, out_ref, acc_ref, s_ref):
    tok = q_ref.shape[0]
    width = q_ref.shape[1]
    half = width // 2
    vsize = gain_ref.shape[1]
    length = kv_ref.shape[0]
    block = s_ref.shape[0]
    q = q_ref[...]
    lane = lax.broadcasted_iota(jnp.int32, q.shape, 1)
    zero = jnp.zeros_like(q)
    both = jnp.concatenate(
        [jnp.where(lane < half, q, zero), jnp.where(lane >= half, q, zero)], axis=0
    ) * jnp.asarray(half ** (-0.5), q.dtype)
    acc_ref[...] = jnp.zeros_like(acc_ref)

    def step(i, state):
        peak, total = state
        kv = kv_ref[pl.ds(i * block, block), :]
        s_ref[...] = lax.dot_general(
            kv[:, :width], both, (((1,), (1,)), ((), ())), preferred_element_type=jnp.float32
        )
        scores = s_ref[...]
        new_peak = jnp.maximum(peak, jnp.max(scores, axis=0, keepdims=True))
        factor = jnp.exp2((peak - new_peak) * log2e)
        expo = jnp.exp2((scores - new_peak) * log2e)
        total = total * factor + jnp.sum(expo, axis=0, keepdims=True)
        acc_ref[...] = acc_ref[...] * factor + lax.dot_general(
            kv[:, width:], expo.astype(jnp.bfloat16), (((0,), (0,)), ((), ())),
            preferred_element_type=jnp.float32,
        )
        return new_peak, total

    peak = jnp.full((1, 2 * tok), -1e30, jnp.float32)
    total = jnp.zeros((1, 2 * tok), jnp.float32)
    peak, total = lax.fori_loop(0, length // block, step, (peak, total))
    mapped = acc_ref[...] / total
    head = mapped[:, :tok] - lam_ref[0, 0] * mapped[:, tok:]
    scaled = head * lax.rsqrt(jnp.mean(head * head, axis=0, keepdims=True) + epsilon)
    out_ref[...] = (jnp.transpose(scaled) * gain_ref[...]).astype(jnp.bfloat16)


def attention(q, kv, lam, gain, block=512):
    tok, vsize = q.shape[0], gain.shape[0]
    vm = pl.BlockSpec(memory_space=pltpu.VMEM)
    return pl.pallas_call(
        attention_kernel,
        out_shape=jax.ShapeDtypeStruct((tok, vsize), jnp.bfloat16),
        in_specs=[vm, vm, pl.BlockSpec(memory_space=pltpu.SMEM), vm],
        out_specs=vm,
        scratch_shapes=[
            pltpu.VMEM((vsize, 2 * tok), jnp.float32),
            pltpu.VMEM((block, 2 * tok), jnp.float32),
        ],
        cost_estimate=pl.CostEstimate(
            flops=8 * tok * kv.shape[0] * vsize, bytes_accessed=kv.size * 2, transcendentals=0
        ),
        name="attention",
    )(q, kv, lam.reshape(1, 1), gain.reshape(1, vsize))


def per_device(
    inputs,
    norm_gain,
    query_weight,
    key_weight,
    value_weight,
    query_gain,
    key_gain,
    mix_lambda,
    head_gain,
    post_gate_weight,
    pre_gate_weight,
    inner_weight,
    conv_taps,
    attn_out_weight,
    conv_out_weight,
):
    tokens = inputs[0]
    tok, feat = tokens.shape
    sp, fs, tp = lax.axis_size("sp"), lax.axis_size("fs"), lax.axis_size("tp")
    half = query_gain.shape[0]
    vsize = head_gain.shape[0]
    channels = post_gate_weight.shape[1]
    tp_index = lax.axis_index("tp")
    lam = lax.dynamic_slice_in_dim(mix_lambda, tp_index, 1)
    taps = lax.dynamic_slice_in_dim(conv_taps, tp_index * channels, channels, 1)

    kv_weight = jnp.concatenate([key_weight, value_weight], axis=1)
    kv_weight = from_everyone(kv_weight, "sp")
    whole = from_everyone(tokens, "tp")
    rest = jnp.concatenate(
        [
            query_weight,
            post_gate_weight,
            pre_gate_weight,
            inner_weight,
            conv_out_weight,
            attn_out_weight,
        ],
        axis=1,
    )
    rest = lax.all_gather(rest, "sp", axis=0, tiled=True)
    kv_weight = kv_weight.reshape(-1, kv_weight.shape[-1])
    kv_weight = rows_in_order(from_everyone(kv_weight, "fs"), sp, fs)

    wide = whole.astype(jnp.float32)
    mean = jnp.mean(wide * wide, axis=(0, 2), keepdims=True)
    normed = (wide * lax.rsqrt(mean + epsilon) * norm_gain.reshape(tp, 1, feat)).astype(jnp.bfloat16)
    normed = jnp.transpose(normed, (1, 0, 2)).reshape(tok, tp * feat)
    key_value = jnp.dot(normed, kv_weight, preferred_element_type=jnp.float32)
    key = scale_rows(key_value[:, : 2 * half].reshape(tok, 2, half), key_gain)
    kv = jnp.concatenate([key.reshape(tok, 2 * half), key_value[:, 2 * half :]], axis=1)
    kv = kv.astype(jnp.bfloat16)
    kv_all = lax.all_gather(kv, "sp", axis=0, tiled=True)

    rest, unused = lax.optimization_barrier((rest, kv))
    first = 2 * half + 3 * channels
    proj_weight = rows_in_order(from_everyone(rest[:, :first], "fs"), sp, fs)
    out_weight = rows_in_order(from_everyone(rest[:, first:], "fs"), sp, fs)
    conv_out, attn_out = out_weight[:, :channels], out_weight[:, channels:]
    attn_out = from_everyone(attn_out, "tp")

    proj = jnp.dot(normed, proj_weight, preferred_element_type=jnp.float32)
    query = scale_rows(proj[:, : 2 * half].reshape(tok, 2, half), query_gain)
    query = query.reshape(tok, 2 * half).astype(jnp.bfloat16)
    at = 2 * half
    post = proj[:, at : at + channels].astype(jnp.bfloat16)
    pre = proj[:, at + channels : at + 2 * channels]
    inner = proj[:, at + 2 * channels :]
    signal = (pre * inner).astype(jnp.bfloat16)
    up = [(i, i + 1) for i in range(sp - 1)]
    before = lax.ppermute(signal[tok - 1 :], "sp", up)
    after = lax.ppermute(signal[:1], "sp", [(j, i) for i, j in up])
    signal = lax.optimization_barrier(signal)
    around = jnp.concatenate([before, signal, after], axis=0).astype(jnp.float32)
    filtered = taps[0] * around[:-2] + taps[1] * around[1:-1] + taps[2] * around[2:]
    conv_hidden = (lax.optimization_barrier(post).astype(jnp.float32) * filtered).astype(jnp.bfloat16)
    contract = (((1,), (1,)), ((), ()))
    conv_part = lax.dot_general(
        conv_hidden, conv_out, contract, preferred_element_type=jnp.float32
    ).astype(jnp.bfloat16)
    conv_part = lax.all_to_all(
        conv_part.reshape(tp, tok // tp, -1), "tp", split_axis=0, concat_axis=0, tiled=True
    )

    hidden = attention(query, kv_all, lam, head_gain)
    hidden = lax.all_to_all(
        hidden.reshape(tp, tok // tp, vsize), "tp", split_axis=0, concat_axis=0, tiled=True
    )
    mixed = lax.dot_general(
        jnp.transpose(hidden, (1, 0, 2)).reshape(tok // tp, tp * vsize),
        jnp.transpose(attn_out, (1, 0, 2)).reshape(-1, tp * vsize),
        contract,
        preferred_element_type=jnp.float32,
    )
    mixed = mixed + conv_part.astype(jnp.float32).sum(axis=0)
    return mixed.astype(jnp.bfloat16)[None]


def solution(mesh):
    weight = P(("sp", "fs"), "tp")
    placed = (P("fs", "sp", "tp"), P(), weight, weight, weight, P(), P(), P(), P())
    placed = placed + (weight, weight, weight, P(), weight, weight)
    return jax.shard_map(
        per_device,
        mesh=mesh,
        in_specs=placed,
        out_specs=P("fs", ("sp", "tp"), None),
        check_vma=False,
    )
```

```python
import jax
import jax.numpy as jnp
from jax import lax
from jax.experimental import pallas as pl
from jax.experimental.pallas import tpu as pltpu
from jax.sharding import PartitionSpec as P

epsilon = 1e-06
log2e = 1.4426950408889634
bf16, f32 = jnp.bfloat16, jnp.float32
vmem = pl.BlockSpec(memory_space=pltpu.VMEM)
smem = pl.BlockSpec(memory_space=pltpu.SMEM)
rows_by_rows = (((1,), (1,)), ((), ()))


def struct(shape, kind):
    return jax.ShapeDtypeStruct(shape, kind)


def dot(a, b):
    return jnp.dot(a, b, preferred_element_type=f32)


def from_everyone(x, axis):
    copies = jnp.broadcast_to(x, (lax.axis_size(axis), *x.shape))
    return lax.all_to_all(copies, axis, split_axis=0, concat_axis=0, tiled=True)


def side_by_side_kernel(*refs):
    at = 0
    for ref in refs[:-1]:
        refs[-1][:, at : at + ref.shape[1]] = ref[...]
        at += ref.shape[1]


def side_by_side(*arrays):
    columns = sum(a.shape[1] for a in arrays)
    return pl.pallas_call(
        side_by_side_kernel,
        out_shape=struct((arrays[0].shape[0], columns), arrays[0].dtype),
        in_specs=[vmem] * len(arrays),
        out_specs=vmem,
        name="side_by_side",
    )(*arrays)


def put_rows_in_order(tiles_ref, first, count, out_ref, piece):
    fs, rows, _ = tiles_ref.shape
    for z in range(rows // piece):
        for y in range(fs):
            at = (z * fs + y) * piece
            out_ref[at : at + piece, :] = tiles_ref[
                y, z * piece : (z + 1) * piece, first : first + count
            ]


def halves_normed(x, gain):
    half = x.shape[1] // 2
    low = lax.broadcasted_iota(jnp.int32, x.shape, 1) < half
    squares = x * x
    zero = jnp.zeros_like(squares)
    one = jnp.sum(jnp.where(low, squares, zero), axis=1, keepdims=True) / half
    two = jnp.sum(jnp.where(low, zero, squares), axis=1, keepdims=True) / half
    return x * jnp.where(low, lax.rsqrt(one + epsilon), lax.rsqrt(two + epsilon)) * gain


def key_value_kernel(x_ref, gain_ref, w_ref, key_gain_ref, normed_ref, kv_ref, rows_ref, piece):
    blocks, tok, feat = x_ref.shape
    put_rows_in_order(w_ref, 0, w_ref.shape[2], rows_ref, piece)
    squares = jnp.zeros((tok, feat), f32)
    for b in range(blocks):
        x = x_ref[b].astype(f32)
        squares = squares + x * x
    mean = jnp.sum(squares, axis=1, keepdims=True) / (blocks * feat)
    scale = lax.rsqrt(mean + epsilon)
    for b in range(blocks):
        normed_ref[:, b * feat : (b + 1) * feat] = (
            x_ref[b].astype(f32) * scale * gain_ref[:, b * feat : (b + 1) * feat]
        ).astype(bf16)
    both = dot(normed_ref[...], rows_ref[...])
    width = key_gain_ref.shape[1]
    kv_ref[:, :width] = halves_normed(both[:, :width], key_gain_ref[...]).astype(bf16)
    kv_ref[:, width:] = both[:, width:].astype(bf16)


def query_kernel(x_ref, w_ref, gain_ref, q_ref, out_w_ref, rows_ref, piece):
    width = gain_ref.shape[1]
    put_rows_in_order(w_ref, 0, width, rows_ref, piece)
    put_rows_in_order(w_ref, width, out_w_ref.shape[1], out_w_ref, piece)
    q_ref[...] = halves_normed(dot(x_ref[...], rows_ref[...]), gain_ref[...]).astype(bf16)


def conv_kernel(
    x_ref, edge_ref, one_ref, two_ref, all_taps_ref, me_ref, part_ref,
    pre_ref, inner_ref, post_ref, signal_ref, at, piece,
):
    tok, channels = x_ref.shape[0], pre_ref.shape[1]
    me = me_ref[0]
    taps = all_taps_ref[:, pl.ds(pl.multiple_of(me * channels, channels), channels)]
    put_rows_in_order(one_ref, at, channels, pre_ref, piece)
    put_rows_in_order(two_ref, 0, channels, inner_ref, piece)
    x = x_ref[...]
    signal = (dot(x, pre_ref[...]) * dot(x, inner_ref[...])).astype(bf16).astype(f32)
    signal_ref[8 : tok + 8, :] = signal
    edge = edge_ref[...]
    side = (dot(edge, pre_ref[...]) * dot(edge, inner_ref[...])).astype(bf16).astype(f32)
    signal_ref[7:8, :] = side[0:1]
    signal_ref[tok + 8 : tok + 9, :] = side[8:9]
    put_rows_in_order(two_ref, channels, channels, post_ref, piece)
    post = dot(x, post_ref[...]).astype(bf16).astype(f32)
    filtered = (
        taps[0:1, :] * signal_ref[7 : tok + 7, :]
        + taps[1:2, :] * signal
        + taps[2:3, :] * signal_ref[9 : tok + 9, :]
    )
    hidden = (post * filtered).astype(bf16)
    put_rows_in_order(two_ref, 2 * channels, channels, pre_ref, piece)
    part = lax.dot_general(
        hidden, pre_ref[...], rows_by_rows, preferred_element_type=f32
    ).astype(bf16)
    _, chips, rows, _ = part_ref.shape
    for t in range(2 * chips):
        ahead = (t // 2 - (me >> 1)) & (chips - 1)
        part_ref[(t % 2) ^ (me & 1), ahead] = part[t * rows : (t + 1) * rows]


def attention_kernel(q_ref, kv_ref, lam_ref, gain_ref, me_ref, out_ref, acc_ref, one_ref, two_ref):
    tok, width = q_ref.shape
    half = width // 2
    length = kv_ref.shape[0]
    block = one_ref.shape[0]
    steps = length // block
    q = q_ref[...]
    lane = lax.broadcasted_iota(jnp.int32, q.shape, 1)
    zero = jnp.zeros_like(q)
    both = jnp.concatenate(
        [jnp.where(lane < half, q, zero), jnp.where(lane >= half, q, zero)], axis=0
    ) * jnp.asarray(half ** (-0.5), q.dtype)
    acc_ref[...] = jnp.zeros_like(acc_ref)

    def scores_of(i, s_ref):
        key = kv_ref[pl.ds(pl.multiple_of(i * block, block), block), :width]
        scores = lax.dot_general(key, both, rows_by_rows, preferred_element_type=f32)
        s_ref[...] = scores
        return jnp.max(scores, axis=0, keepdims=True)

    def take(i, s_ref, top, state):
        peak, total = state
        new_peak = jnp.maximum(peak, top)
        factor = jnp.exp2((peak - new_peak) * log2e)
        expo = jnp.exp2((s_ref[...] - new_peak) * log2e)
        total = total * factor + jnp.sum(expo, axis=0, keepdims=True)
        value = kv_ref[pl.ds(pl.multiple_of(i * block, block), block), width:]
        acc_ref[...] = acc_ref[...] * factor + lax.dot_general(
            value, expo.astype(bf16), (((0,), (0,)), ((), ())), preferred_element_type=f32
        )
        return new_peak, total

    def step(j, carry):
        top, state = carry
        next_top = scores_of(2 * j + 1, two_ref)
        state = take(2 * j, one_ref, top, state)
        top = scores_of(jnp.minimum(2 * j + 2, steps - 1), one_ref)
        state = take(2 * j + 1, two_ref, next_top, state)
        return top, state

    peak = jnp.full((1, 2 * tok), -1e30, f32)
    total = jnp.zeros((1, 2 * tok), f32)
    top = scores_of(0, one_ref)
    _, (peak, total) = lax.fori_loop(0, steps // 2, step, (top, (peak, total)))
    mapped = acc_ref[...] / total
    head = mapped[:, :tok] - lam_ref[me_ref[0]] * mapped[:, tok:]
    scaled = head * lax.rsqrt(jnp.mean(head * head, axis=0, keepdims=True) + epsilon)
    out_ref[...] = (jnp.transpose(scaled) * gain_ref[...]).astype(bf16)


def final_kernel(hidden_ref, own_ref, pair_ref, mine_ref, *refs):
    me_ref, out_ref = refs[-2:]
    me = me_ref[0]
    total = mine_ref[...].astype(f32)
    for ref in refs[:-2]:
        total = total + ref[...].astype(f32)
    chips = own_ref.shape[0]
    for d in range(chips):
        source = 2 * (((me >> 1) - d) & (chips - 1)) + (me & 1)
        for k, w_ref in enumerate((own_ref, pair_ref)):
            total = total + lax.dot_general(
                hidden_ref[source ^ k], w_ref[d], rows_by_rows, preferred_element_type=f32
            )
    out_ref[...] = total.astype(bf16)


def per_device(
    inputs,
    norm_gain,
    query_weight,
    key_weight,
    value_weight,
    query_gain,
    key_gain,
    mix_lambda,
    head_gain,
    post_gate_weight,
    pre_gate_weight,
    inner_weight,
    conv_taps,
    attn_out_weight,
    conv_out_weight,
):
    tokens = inputs[0]
    tok, feat = tokens.shape
    sp, tp = lax.axis_size("sp"), lax.axis_size("tp")
    total_feat = tp * feat
    width = key_weight.shape[1]
    vsize = head_gain.shape[0]
    channels = post_gate_weight.shape[1]
    piece = key_weight.shape[0]
    out_rows = tok // tp
    chips = tp // 2
    me = lax.axis_index("tp").astype(jnp.int32).reshape(1)
    key_gain_2 = jnp.tile(key_gain, 2).reshape(1, width)
    query_gain_2 = jnp.tile(query_gain, 2).reshape(1, width)

    whole = lax.all_gather(tokens, "tp", axis=0, tiled=False)
    first = side_by_side(
        key_weight, value_weight, query_weight, attn_out_weight, pre_gate_weight
    )
    first = lax.all_gather(first, "sp", axis=0, tiled=True)
    kv_weight = from_everyone(first[:, : width + vsize], "fs")
    normed, kv = pl.pallas_call(
        lambda *refs: key_value_kernel(*refs, piece=piece),
        out_shape=(struct((tok, total_feat), bf16), struct((tok, width + vsize), bf16)),
        in_specs=[vmem] * 4,
        out_specs=(vmem, vmem),
        scratch_shapes=[pltpu.VMEM((total_feat, width + vsize), bf16)],
        name="key_value",
    )(whole, norm_gain.reshape(1, total_feat), kv_weight, key_gain_2)
    kv_all = lax.all_gather(kv, "sp", axis=0, tiled=True)

    up = [(i, i + 1) for i in range(sp - 1)]
    before = lax.ppermute(normed[tok - 8 :], "sp", up)
    after = lax.ppermute(normed[:8], "sp", [(j, i) for i, j in up])
    edge = jnp.concatenate([before[7:], before[:7], after], axis=0)

    one, _ = lax.optimization_barrier((first[:, width + vsize :], kv_weight))
    one = from_everyone(one, "fs")
    second = side_by_side(inner_weight, post_gate_weight, conv_out_weight)
    second, _ = lax.optimization_barrier((second, kv))
    second = lax.all_gather(second, "sp", axis=0, tiled=True)
    query, attn_out = pl.pallas_call(
        lambda *refs: query_kernel(*refs, piece=piece),
        out_shape=(struct((tok, width), bf16), struct((total_feat, vsize), bf16)),
        in_specs=[vmem] * 3,
        out_specs=(vmem, vmem),
        scratch_shapes=[pltpu.VMEM((total_feat, width), bf16)],
        name="query",
    )(normed, one, query_gain_2)

    def shifted(x, d):
        return lax.ppermute(x, "tp", [(i, (i + 2 * d) % tp) for i in range(tp)])

    def to_pair(x):
        return lax.ppermute(x, "tp", [(i, i ^ 1) for i in range(tp)])

    own = jnp.stack([attn_out] + [shifted(attn_out, d) for d in range(1, chips)])
    pair = to_pair(own)
    two = from_everyone(second, "fs")
    part = pl.pallas_call(
        lambda *refs: conv_kernel(*refs, at=width + vsize, piece=piece),
        out_shape=struct((2, chips, out_rows, total_feat), bf16),
        in_specs=[vmem] * 5 + [smem],
        out_specs=vmem,
        scratch_shapes=[pltpu.VMEM((total_feat, channels), bf16) for _ in range(3)]
        + [pltpu.VMEM((tok + 16, channels), f32)],
        name="conv",
    )(normed, edge, one, two, conv_taps, me)
    part = (part[0].astype(f32) + to_pair(part[1]).astype(f32)).astype(bf16)
    arrived = [shifted(part[d], d) for d in range(1, chips)]

    hidden = pl.pallas_call(
        attention_kernel,
        out_shape=struct((tok, vsize), bf16),
        in_specs=[vmem, vmem, smem, vmem, smem],
        out_specs=vmem,
        scratch_shapes=[pltpu.VMEM((vsize, 2 * tok), f32)] + [pltpu.VMEM((512, 2 * tok), f32)] * 2,
        cost_estimate=pl.CostEstimate(
            flops=8 * tok * kv_all.shape[0] * vsize, bytes_accessed=kv_all.size * 2, transcendentals=0
        ),
        name="attention",
    )(query, kv_all, mix_lambda, head_gain.reshape(1, vsize), me)
    hidden = lax.all_to_all(
        hidden.reshape(tp, out_rows, vsize), "tp", split_axis=0, concat_axis=0, tiled=True
    )
    return pl.pallas_call(
        final_kernel,
        out_shape=struct((out_rows, total_feat), bf16),
        in_specs=[vmem] * (4 + len(arrived)) + [smem],
        out_specs=vmem,
        name="final",
    )(hidden, own, pair, part[0], *arrived, me)[None]


def solution(mesh):
    weight = P(("sp", "fs"), "tp")
    placed = (P("fs", "sp", "tp"), P(), weight, weight, weight, P(), P(), P(), P())
    placed = placed + (weight, weight, weight, P(), weight, weight)
    return jax.shard_map(
        per_device,
        mesh=mesh,
        in_specs=placed,
        out_specs=P("fs", ("sp", "tp"), None),
        check_vma=False,
    )
```

```python
import jax
import jax.numpy as jnp
from jax import lax
from jax.experimental import pallas as pl
from jax.experimental.pallas import tpu as pltpu
from jax.sharding import PartitionSpec as P

epsilon = 1e-06
log2e = 1.4426950408889634
bf16, f32 = jnp.bfloat16, jnp.float32
vmem = pl.BlockSpec(memory_space=pltpu.VMEM)
smem = pl.BlockSpec(memory_space=pltpu.SMEM)
rows_by_rows = (((1,), (1,)), ((), ()))


def struct(shape, kind):
    return jax.ShapeDtypeStruct(shape, kind)


def dot(a, b):
    return jnp.dot(a, b, preferred_element_type=f32)


def from_everyone(x, axis):
    copies = jnp.broadcast_to(x, (lax.axis_size(axis), *x.shape))
    return lax.all_to_all(copies, axis, split_axis=0, concat_axis=0, tiled=True)


def side_by_side_kernel(*refs):
    at = 0
    for ref in refs[:-1]:
        refs[-1][:, at : at + ref.shape[1]] = ref[...]
        at += ref.shape[1]


def side_by_side(*arrays):
    columns = sum(a.shape[1] for a in arrays)
    return pl.pallas_call(
        side_by_side_kernel,
        out_shape=struct((arrays[0].shape[0], columns), arrays[0].dtype),
        in_specs=[vmem] * len(arrays),
        out_specs=vmem,
        name="side_by_side",
    )(*arrays)


def put_rows_in_order(tiles_ref, first, count, out_ref, piece):
    fs, rows, _ = tiles_ref.shape
    for z in range(rows // piece):
        for y in range(fs):
            at = (z * fs + y) * piece
            out_ref[at : at + piece, :] = tiles_ref[
                y, z * piece : (z + 1) * piece, first : first + count
            ]


def halves_normed(x, gain):
    half = x.shape[1] // 2
    low = lax.broadcasted_iota(jnp.int32, x.shape, 1) < half
    squares = x * x
    zero = jnp.zeros_like(squares)
    one = jnp.sum(jnp.where(low, squares, zero), axis=1, keepdims=True) / half
    two = jnp.sum(jnp.where(low, zero, squares), axis=1, keepdims=True) / half
    return x * jnp.where(low, lax.rsqrt(one + epsilon), lax.rsqrt(two + epsilon)) * gain


def key_value_kernel(x_ref, gain_ref, w_ref, key_gain_ref, normed_ref, kv_ref, rows_ref, piece):
    blocks, tok, feat = x_ref.shape
    put_rows_in_order(w_ref, 0, w_ref.shape[2], rows_ref, piece)
    squares = jnp.zeros((tok, feat), f32)
    for b in range(blocks):
        x = x_ref[b].astype(f32)
        squares = squares + x * x
    mean = jnp.sum(squares, axis=1, keepdims=True) / (blocks * feat)
    scale = lax.rsqrt(mean + epsilon)
    for b in range(blocks):
        normed_ref[:, b * feat : (b + 1) * feat] = (
            x_ref[b].astype(f32) * scale * gain_ref[:, b * feat : (b + 1) * feat]
        ).astype(bf16)
    both = dot(normed_ref[...], rows_ref[...])
    width = key_gain_ref.shape[1]
    kv_ref[:, :width] = halves_normed(both[:, :width], key_gain_ref[...]).astype(bf16)
    kv_ref[:, width:] = both[:, width:].astype(bf16)


def query_kernel(
    x_ref, edge_ref, w_ref, gain_ref, all_taps_ref, me_ref, q_ref, filtered_ref, rows_ref, signal_ref,
    piece,
):
    tok, channels = filtered_ref.shape
    width = gain_ref.shape[1]
    put_rows_in_order(w_ref, 0, w_ref.shape[2], rows_ref, piece)
    x = x_ref[...]
    q_ref[...] = halves_normed(dot(x, rows_ref[:, :width]), gain_ref[...]).astype(bf16)

    def signal_of(rows):
        both = dot(rows, rows_ref[:, width:])
        return (both[:, :channels] * both[:, channels:]).astype(bf16).astype(f32)

    signal = signal_of(x)
    side = signal_of(edge_ref[...])
    signal_ref[8 : tok + 8, :] = signal
    signal_ref[7:8, :] = side[0:1]
    signal_ref[tok + 8 : tok + 9, :] = side[8:9]
    taps = all_taps_ref[:, pl.ds(pl.multiple_of(me_ref[0] * channels, channels), channels)]
    filtered_ref[...] = (
        taps[0:1, :] * signal_ref[7 : tok + 7, :]
        + taps[1:2, :] * signal
        + taps[2:3, :] * signal_ref[9 : tok + 9, :]
    )


def conv_kernel(x_ref, filtered_ref, w_ref, hidden_ref, out_w_ref, rows_ref, piece):
    channels = filtered_ref.shape[1]
    put_rows_in_order(w_ref, 0, channels, rows_ref, piece)
    put_rows_in_order(w_ref, channels, out_w_ref.shape[1], out_w_ref, piece)
    post = dot(x_ref[...], rows_ref[...]).astype(bf16).astype(f32)
    hidden_ref[...] = (post * filtered_ref[...]).astype(bf16)


def attention_kernel(
    q_ref, kv_ref, lam_ref, gain_ref, conv_ref, out_w_ref, me_ref, mine_ref, theirs_ref,
    acc_ref, one_ref, two_ref, all_ref, sems,
):
    tok, width = q_ref.shape
    half = width // 2
    length = kv_ref.shape[0]
    block = one_ref.shape[0]
    steps = length // block
    me = me_ref[0]
    early = 3 * block

    def arrival(start, size, k):
        rows = pl.ds(start, size)
        return pltpu.make_async_copy(kv_ref.at[rows], all_ref.at[rows], sems.at[k])

    head, tail = arrival(0, early, 0), arrival(early, length - early, 1)
    head.start()
    tail.start()
    q = q_ref[...].astype(f32) * (log2e * half ** (-0.5))
    high = q.astype(bf16)
    low = (q - high.astype(f32)).astype(bf16)
    lane = lax.broadcasted_iota(jnp.int32, q.shape, 1)
    zero = jnp.zeros_like(high)
    both = jnp.concatenate(
        [
            jnp.concatenate([jnp.where(mask, high, zero), jnp.where(mask, low, zero)], axis=1)
            for mask in (lane < half, lane >= half)
        ],
        axis=0,
    )
    acc_ref[...] = jnp.zeros_like(acc_ref)

    def rows_of(i):
        return pl.ds(pl.multiple_of(i * block, block), block)

    def scores_of(i, s_ref):
        key = all_ref[rows_of(i), :width]
        scores = lax.dot_general(
            jnp.concatenate([key, key], axis=1), both, rows_by_rows, preferred_element_type=f32
        )
        s_ref[...] = scores
        return jnp.max(scores, axis=0, keepdims=True)

    def take(i, s_ref, top, state):
        peak, total = state
        new_peak = jnp.maximum(peak, top)
        factor = jnp.exp2(peak - new_peak)
        expo = jnp.exp2(s_ref[...] - new_peak)
        total = total * factor + jnp.sum(expo, axis=0, keepdims=True)
        acc_ref[...] = acc_ref[...] * factor + lax.dot_general(
            all_ref[rows_of(i), width:], expo.astype(bf16), (((0,), (0,)), ((), ())),
            preferred_element_type=f32,
        )
        return new_peak, total

    def step(j, carry):
        @pl.when(j == 1)
        def _():
            tail.wait()

        top, state = carry
        next_top = scores_of(2 * j + 1, two_ref)
        state = take(2 * j, one_ref, top, state)
        top = scores_of(jnp.minimum(2 * j + 2, steps - 1), one_ref)
        state = take(2 * j + 1, two_ref, next_top, state)
        return top, state

    peak = jnp.full((1, 2 * tok), -1e30, f32)
    total = jnp.zeros((1, 2 * tok), f32)
    head.wait()
    top = scores_of(0, one_ref)
    _, (peak, total) = lax.fori_loop(0, steps // 2, step, (top, (peak, total)))
    mapped = acc_ref[...] / total
    out = mapped[:, :tok] - lam_ref[me] * mapped[:, tok:]
    scaled = out * lax.rsqrt(jnp.mean(out * out, axis=0, keepdims=True) + epsilon)
    hidden = (jnp.transpose(scaled) * gain_ref[...]).astype(bf16)
    channels = conv_ref.shape[1]
    part = lax.dot_general(
        conv_ref[...], out_w_ref[:, :channels], rows_by_rows, preferred_element_type=f32
    ) + lax.dot_general(hidden, out_w_ref[:, channels:], rows_by_rows, preferred_element_type=f32)
    chips, rows, _ = mine_ref.shape
    first_core = (me & 1) == 0
    for chip in range(chips):
        one = part[2 * chip * rows : (2 * chip + 1) * rows]
        two = part[(2 * chip + 1) * rows : (2 * chip + 2) * rows]
        mine_ref[chip] = jnp.where(first_core, one, two).astype(bf16)
        theirs_ref[chip] = jnp.where(first_core, two, one).astype(bf16)


def per_device(
    inputs,
    norm_gain,
    query_weight,
    key_weight,
    value_weight,
    query_gain,
    key_gain,
    mix_lambda,
    head_gain,
    post_gate_weight,
    pre_gate_weight,
    inner_weight,
    conv_taps,
    attn_out_weight,
    conv_out_weight,
):
    tokens = inputs[0]
    tok, feat = tokens.shape
    sp, tp = lax.axis_size("sp"), lax.axis_size("tp")
    total_feat = tp * feat
    width = key_weight.shape[1]
    vsize = head_gain.shape[0]
    channels = post_gate_weight.shape[1]
    piece = key_weight.shape[0]
    out_rows = tok // tp
    chips = tp // 2
    me = lax.axis_index("tp").astype(jnp.int32).reshape(1)
    key_gain_2 = jnp.tile(key_gain, 2).reshape(1, width)
    query_gain_2 = jnp.tile(query_gain, 2).reshape(1, width)

    whole = lax.all_gather(tokens, "tp", axis=0, tiled=False)
    first = side_by_side(
        key_weight, value_weight, query_weight, pre_gate_weight, inner_weight
    )
    first = lax.all_gather(first, "sp", axis=0, tiled=True)
    kv_weight = from_everyone(first[:, : width + vsize], "fs")
    normed, kv = pl.pallas_call(
        lambda *refs: key_value_kernel(*refs, piece=piece),
        out_shape=(struct((tok, total_feat), bf16), struct((tok, width + vsize), bf16)),
        in_specs=[vmem] * 4,
        out_specs=(vmem, vmem),
        scratch_shapes=[pltpu.VMEM((total_feat, width + vsize), bf16)],
        name="key_value",
    )(whole, norm_gain.reshape(1, total_feat), kv_weight, key_gain_2)
    kv_all = lax.all_gather(kv, "sp", axis=0, tiled=True)

    up = [(i, i + 1) for i in range(sp - 1)]
    before = lax.ppermute(normed[tok - 8 :], "sp", up)
    after = lax.ppermute(normed[:8], "sp", [(j, i) for i, j in up])
    edge = jnp.concatenate([before[7:], before[:7], after], axis=0)

    one, _ = lax.optimization_barrier((first[:, width + vsize :], kv_weight))
    one = from_everyone(one, "fs")
    second = side_by_side(post_gate_weight, conv_out_weight, attn_out_weight)
    second, _ = lax.optimization_barrier((second, kv))
    second = lax.all_gather(second, "sp", axis=0, tiled=True)
    query, filtered = pl.pallas_call(
        lambda *refs: query_kernel(*refs, piece=piece),
        out_shape=(struct((tok, width), bf16), struct((tok, channels), f32)),
        in_specs=[vmem] * 5 + [smem],
        out_specs=(vmem, vmem),
        scratch_shapes=[
            pltpu.VMEM((total_feat, width + 2 * channels), bf16),
            pltpu.VMEM((tok + 16, channels), f32),
        ],
        name="query",
    )(normed, edge, one, query_gain_2, conv_taps, me)

    two = from_everyone(second, "fs")
    conv_hidden, out_weight = pl.pallas_call(
        lambda *refs: conv_kernel(*refs, piece=piece),
        out_shape=(struct((tok, channels), bf16), struct((total_feat, channels + vsize), bf16)),
        in_specs=[vmem] * 3,
        out_specs=(vmem, vmem),
        scratch_shapes=[pltpu.VMEM((total_feat, channels), bf16)],
        name="conv",
    )(normed, filtered, two)

    mine, theirs = pl.pallas_call(
        attention_kernel,
        out_shape=(struct((chips, out_rows, total_feat), bf16),) * 2,
        in_specs=[vmem, pl.BlockSpec(memory_space=pl.ANY), smem, vmem, vmem, vmem, smem],
        out_specs=(vmem, vmem),
        scratch_shapes=[pltpu.VMEM((vsize, 2 * tok), f32)]
        + [pltpu.VMEM((512, 2 * tok), f32)] * 2
        + [pltpu.VMEM(kv_all.shape, bf16), pltpu.SemaphoreType.DMA((2,))],
        cost_estimate=pl.CostEstimate(
            flops=8 * tok * kv_all.shape[0] * vsize, bytes_accessed=kv_all.size * 2, transcendentals=0
        ),
        name="attention",
    )(query, kv_all, mix_lambda, head_gain.reshape(1, vsize), conv_hidden, out_weight, me)
    theirs = lax.ppermute(theirs, "tp", [(i, i ^ 1) for i in range(tp)])
    part = (mine.astype(f32) + theirs.astype(f32)).astype(bf16)
    same_core = [list(range(c, tp, 2)) for c in range(2)]
    arrived = lax.all_to_all(
        part, "tp", split_axis=0, concat_axis=0, tiled=True, axis_index_groups=same_core
    )
    return jnp.sum(arrived.astype(f32), axis=0).astype(bf16)[None]


def solution(mesh):
    weight = P(("sp", "fs"), "tp")
    placed = (P("fs", "sp", "tp"), P(), weight, weight, weight, P(), P(), P(), P())
    placed = placed + (weight, weight, weight, P(), weight, weight)
    return jax.shard_map(
        per_device,
        mesh=mesh,
        in_specs=placed,
        out_specs=P("fs", ("sp", "tp"), None),
        check_vma=False,
    )
```

```python
import jax
import jax.numpy as jnp
from jax import lax
from jax.experimental import pallas as pl
from jax.experimental.pallas import tpu as pltpu
from jax.sharding import PartitionSpec as P

epsilon = 1e-06
log2e = 1.4426950408889634
bf16, f32 = jnp.bfloat16, jnp.float32
vmem = pl.BlockSpec(memory_space=pltpu.VMEM)
smem = pl.BlockSpec(memory_space=pltpu.SMEM)
rows_by_rows = (((1,), (1,)), ((), ()))


def struct(shape, kind):
    return jax.ShapeDtypeStruct(shape, kind)


def dot(a, b):
    return jnp.dot(a, b, preferred_element_type=f32)


def from_everyone(x, axis):
    copies = jnp.broadcast_to(x, (lax.axis_size(axis), *x.shape))
    return lax.all_to_all(copies, axis, split_axis=0, concat_axis=0, tiled=True)


def side_by_side_kernel(*refs):
    at = 0
    for ref in refs[:-1]:
        refs[-1][:, at : at + ref.shape[1]] = ref[...]
        at += ref.shape[1]


def side_by_side(*arrays):
    columns = sum(a.shape[1] for a in arrays)
    return pl.pallas_call(
        side_by_side_kernel,
        out_shape=struct((arrays[0].shape[0], columns), arrays[0].dtype),
        in_specs=[vmem] * len(arrays),
        out_specs=vmem,
        name="side_by_side",
    )(*arrays)


def start_rows(w_ref, first, count, out_ref, sems):
    copies = []
    for y in range(w_ref.shape[0]):
        copies.append(
            pltpu.make_async_copy(
                w_ref.at[y, :, :, pl.ds(first, count)], out_ref.at[:, y], sems.at[y]
            )
        )
        copies[-1].start()
    return copies


def wait_rows(copies, out_ref):
    for copy in copies:
        copy.wait()
    sp, fs, piece, n = out_ref.shape
    return out_ref[...].reshape(sp * fs * piece, n)


def twice(gain_ref):
    return jnp.concatenate([gain_ref[...], gain_ref[...]], axis=1)


def halves_normed(x, gain):
    half = x.shape[1] // 2
    low = lax.broadcasted_iota(jnp.int32, x.shape, 1) < half
    squares = x * x
    zero = jnp.zeros_like(squares)
    one = jnp.sum(jnp.where(low, squares, zero), axis=1, keepdims=True) / half
    two = jnp.sum(jnp.where(low, zero, squares), axis=1, keepdims=True) / half
    return x * jnp.where(low, lax.rsqrt(one + epsilon), lax.rsqrt(two + epsilon)) * gain


def key_value_kernel(
    x_ref, gain_ref, w_ref, key_gain_ref, normed_ref, kv_ref,
    wide_ref, narrow_ref, rows_ref, in_sems, w_sems, out_sems,
):
    blocks, tok, feat = x_ref.shape
    arrivals = [
        pltpu.make_async_copy(x_ref.at[b], wide_ref.at[b], in_sems.at[b]) for b in range(blocks)
    ]
    for copy in arrivals:
        copy.start()
    copies = start_rows(w_ref, 0, w_ref.shape[3], rows_ref, w_sems)
    squares = jnp.zeros((tok, feat), f32)
    for b in range(blocks):
        arrivals[b].wait()
        x = wide_ref[b].astype(f32)
        squares = squares + x * x
    mean = jnp.sum(squares, axis=1, keepdims=True) / (blocks * feat)
    scale = lax.rsqrt(mean + epsilon)
    leaving = []
    for b in range(blocks):
        columns = pl.ds(b * feat, feat)
        narrow_ref[:, columns] = (
            wide_ref[b].astype(f32) * scale * gain_ref[:, columns]
        ).astype(bf16)
        leaving.append(
            pltpu.make_async_copy(
                narrow_ref.at[:, columns], normed_ref.at[:, columns], out_sems.at[b]
            )
        )
        leaving[-1].start()
    both = dot(narrow_ref[...], wait_rows(copies, rows_ref))
    width = 2 * key_gain_ref.shape[1]
    kv_ref[:, :width] = halves_normed(both[:, :width], twice(key_gain_ref)).astype(bf16)
    kv_ref[:, width:] = both[:, width:].astype(bf16)
    for copy in leaving:
        copy.wait()


def query_kernel(
    x_ref, edge_ref, w_ref, gain_ref, all_taps_ref, me_ref, q_ref, filtered_ref,
    rows_ref, signal_ref, sems,
):
    tok, channels = filtered_ref.shape
    width = 2 * gain_ref.shape[1]
    weights = wait_rows(start_rows(w_ref, 0, w_ref.shape[3], rows_ref, sems), rows_ref)
    x = x_ref[...]
    q_ref[...] = halves_normed(dot(x, weights[:, :width]), twice(gain_ref)).astype(bf16)

    def signal_of(rows):
        both = dot(rows, weights[:, width:])
        return (both[:, :channels] * both[:, channels:]).astype(bf16).astype(f32)

    signal = signal_of(x)
    side = signal_of(edge_ref[...])
    signal_ref[8 : tok + 8, :] = signal
    signal_ref[7:8, :] = side[0:1]
    signal_ref[tok + 8 : tok + 9, :] = side[8:9]
    taps = all_taps_ref[:, pl.ds(pl.multiple_of(me_ref[0] * channels, channels), channels)]
    filtered_ref[...] = (
        taps[0:1, :] * signal_ref[7 : tok + 7, :]
        + taps[1:2, :] * signal
        + taps[2:3, :] * signal_ref[9 : tok + 9, :]
    )


def conv_kernel(x_ref, filtered_ref, w_ref, hidden_ref, rows_ref, sems):
    copies = start_rows(w_ref, 0, filtered_ref.shape[1], rows_ref, sems)
    post = dot(x_ref[...], wait_rows(copies, rows_ref)).astype(bf16).astype(f32)
    hidden_ref[...] = (post * filtered_ref[...]).astype(bf16)


def attention_kernel(
    q_ref, kv_ref, lam_ref, gain_ref, conv_ref, out_w_ref, me_ref, mine_ref, theirs_ref,
    acc_ref, one_ref, two_ref, all_ref, conv_in_ref, rows_ref, sems, w_sems,
):
    tok, width = q_ref.shape
    half = width // 2
    length = kv_ref.shape[0]
    block = one_ref.shape[0]
    steps = length // block
    me = me_ref[0]
    early = 3 * block

    def arrival(start, size, k):
        rows = pl.ds(start, size)
        return pltpu.make_async_copy(kv_ref.at[rows], all_ref.at[rows], sems.at[k])

    head, tail = arrival(0, early, 0), arrival(early, length - early, 1)
    head.start()
    tail.start()
    channels = conv_ref.shape[1]
    conv_copy = pltpu.make_async_copy(conv_ref, conv_in_ref, sems.at[2])
    conv_copy.start()
    copies = start_rows(out_w_ref, channels, rows_ref.shape[3], rows_ref, w_sems)
    q = q_ref[...].astype(f32) * (log2e * half ** (-0.5))
    high = q.astype(bf16)
    low = (q - high.astype(f32)).astype(bf16)
    lane = lax.broadcasted_iota(jnp.int32, q.shape, 1)
    zero = jnp.zeros_like(high)
    both = jnp.concatenate(
        [
            jnp.concatenate([jnp.where(mask, high, zero), jnp.where(mask, low, zero)], axis=1)
            for mask in (lane < half, lane >= half)
        ],
        axis=0,
    )
    acc_ref[...] = jnp.zeros_like(acc_ref)

    def rows_of(i):
        return pl.ds(pl.multiple_of(i * block, block), block)

    def scores_of(i, s_ref):
        key = all_ref[rows_of(i), :width]
        scores = lax.dot_general(
            jnp.concatenate([key, key], axis=1), both, rows_by_rows, preferred_element_type=f32
        )
        s_ref[...] = scores
        return jnp.max(scores, axis=0, keepdims=True)

    def take(i, s_ref, top, state):
        peak, total = state
        new_peak = jnp.maximum(peak, top)
        factor = jnp.exp2(peak - new_peak)
        expo = jnp.exp2(s_ref[...] - new_peak)
        total = total * factor + jnp.sum(expo, axis=0, keepdims=True)
        acc_ref[...] = acc_ref[...] * factor + lax.dot_general(
            all_ref[rows_of(i), width:], expo.astype(bf16), (((0,), (0,)), ((), ())),
            preferred_element_type=f32,
        )
        return new_peak, total

    def step(j, carry):
        @pl.when(j == 1)
        def _():
            tail.wait()

        top, state = carry
        next_top = scores_of(2 * j + 1, two_ref)
        state = take(2 * j, one_ref, top, state)
        top = scores_of(jnp.minimum(2 * j + 2, steps - 1), one_ref)
        state = take(2 * j + 1, two_ref, next_top, state)
        return top, state

    peak = jnp.full((1, 2 * tok), -1e30, f32)
    total = jnp.zeros((1, 2 * tok), f32)
    head.wait()
    top = scores_of(0, one_ref)
    _, (peak, total) = lax.fori_loop(0, steps // 2, step, (top, (peak, total)))
    mapped = acc_ref[...] / total
    out = mapped[:, :tok] - lam_ref[me] * mapped[:, tok:]
    scaled = out * lax.rsqrt(jnp.mean(out * out, axis=0, keepdims=True) + epsilon)
    hidden = (jnp.transpose(scaled) * gain_ref[...]).astype(bf16)
    weights = wait_rows(copies, rows_ref)
    conv_copy.wait()
    part = lax.dot_general(
        jnp.concatenate([conv_in_ref[...], hidden], axis=1), weights, rows_by_rows,
        preferred_element_type=f32,
    )
    chips, rows, _ = mine_ref.shape
    first_core = (me & 1) == 0
    for chip in range(chips):
        one = part[2 * chip * rows : (2 * chip + 1) * rows]
        two = part[(2 * chip + 1) * rows : (2 * chip + 2) * rows]
        mine_ref[chip] = jnp.where(first_core, one, two).astype(bf16)
        theirs_ref[chip] = jnp.where(first_core, two, one).astype(bf16)


def per_device(
    inputs,
    norm_gain,
    query_weight,
    key_weight,
    value_weight,
    query_gain,
    key_gain,
    mix_lambda,
    head_gain,
    post_gate_weight,
    pre_gate_weight,
    inner_weight,
    conv_taps,
    attn_out_weight,
    conv_out_weight,
):
    tokens = inputs[0]
    tok, feat = tokens.shape
    sp, tp = lax.axis_size("sp"), lax.axis_size("tp")
    total_feat = tp * feat
    width = key_weight.shape[1]
    vsize = head_gain.shape[0]
    channels = post_gate_weight.shape[1]
    piece = key_weight.shape[0]
    out_rows = tok // tp
    chips = tp // 2
    me = lax.axis_index("tp").astype(jnp.int32).reshape(1)
    key_gain, query_gain = key_gain.reshape(1, -1), query_gain.reshape(1, -1)
    in_hbm = pl.BlockSpec(memory_space=pl.ANY)

    def by_rows(tiles):
        return tiles.reshape(tiles.shape[0], sp, piece, tiles.shape[2])

    def ordered(columns):
        return pltpu.VMEM((sp, total_feat // (sp * piece), piece, columns), bf16)

    def sems(count):
        return pltpu.SemaphoreType.DMA((count,))

    fs = lax.axis_size("fs")

    whole = lax.all_gather(tokens, "tp", axis=0, tiled=False)
    first = side_by_side(
        key_weight, value_weight, query_weight, pre_gate_weight, inner_weight
    )
    first = lax.all_gather(first, "sp", axis=0, tiled=True)
    kv_weight = from_everyone(first[:, : width + vsize], "fs")
    normed, kv = pl.pallas_call(
        key_value_kernel,
        out_shape=(struct((tok, total_feat), bf16), struct((tok, width + vsize), bf16)),
        in_specs=[in_hbm, vmem, in_hbm, vmem],
        out_specs=(in_hbm, vmem),
        scratch_shapes=[
            pltpu.VMEM((tp, tok, feat), bf16),
            pltpu.VMEM((tok, total_feat), bf16),
            ordered(width + vsize),
            sems(tp),
            sems(fs),
            sems(tp),
        ],
        name="key_value",
    )(whole, norm_gain.reshape(1, total_feat), by_rows(kv_weight), key_gain)
    kv_all = lax.all_gather(kv, "sp", axis=0, tiled=True)

    up = [(i, i + 1) for i in range(sp - 1)]
    before = lax.ppermute(normed[tok - 8 :], "sp", up)
    after = lax.ppermute(normed[:8], "sp", [(j, i) for i, j in up])
    edge = jnp.concatenate([before[7:], before[:7], after], axis=0)

    one, _ = lax.optimization_barrier((first[:, width + vsize :], kv_weight))
    one = from_everyone(one, "fs")
    second = side_by_side(post_gate_weight, conv_out_weight, attn_out_weight)
    second, _ = lax.optimization_barrier((second, kv))
    second = lax.all_gather(second, "sp", axis=0, tiled=True)
    query, filtered = pl.pallas_call(
        query_kernel,
        out_shape=(struct((tok, width), bf16), struct((tok, channels), f32)),
        in_specs=[vmem, vmem, in_hbm, vmem, vmem, smem],
        out_specs=(vmem, vmem),
        scratch_shapes=[
            ordered(width + 2 * channels),
            pltpu.VMEM((tok + 16, channels), f32),
            sems(fs),
        ],
        name="query",
    )(normed, edge, by_rows(one), query_gain, conv_taps, me)

    two = by_rows(from_everyone(second, "fs"))
    conv_hidden = pl.pallas_call(
        conv_kernel,
        out_shape=struct((tok, channels), bf16),
        in_specs=[vmem, vmem, in_hbm],
        out_specs=vmem,
        scratch_shapes=[ordered(channels), sems(fs)],
        name="conv",
    )(normed, filtered, two)

    mine, theirs = pl.pallas_call(
        attention_kernel,
        out_shape=(struct((chips, out_rows, total_feat), bf16),) * 2,
        in_specs=[vmem, in_hbm, smem, vmem, in_hbm, in_hbm, smem],
        out_specs=(vmem, vmem),
        scratch_shapes=[pltpu.VMEM((vsize, 2 * tok), f32)]
        + [pltpu.VMEM((512, 2 * tok), f32)] * 2
        + [pltpu.VMEM(kv_all.shape, bf16), pltpu.VMEM((tok, channels), bf16)]
        + [ordered(channels + vsize), sems(3), sems(fs)],
        cost_estimate=pl.CostEstimate(
            flops=8 * tok * kv_all.shape[0] * vsize, bytes_accessed=kv_all.size * 2, transcendentals=0
        ),
        name="attention",
    )(query, kv_all, mix_lambda, head_gain.reshape(1, vsize), conv_hidden, two, me)
    theirs = lax.ppermute(theirs, "tp", [(i, i ^ 1) for i in range(tp)])
    part = (mine.astype(f32) + theirs.astype(f32)).astype(bf16)
    same_core = [list(range(c, tp, 2)) for c in range(2)]
    arrived = lax.all_to_all(
        part, "tp", split_axis=0, concat_axis=0, tiled=True, axis_index_groups=same_core
    )
    return jnp.sum(arrived.astype(f32), axis=0).astype(bf16)[None]


def solution(mesh):
    weight = P(("sp", "fs"), "tp")
    placed = (P("fs", "sp", "tp"), P(), weight, weight, weight, P(), P(), P(), P())
    placed = placed + (weight, weight, weight, P(), weight, weight)
    return jax.shard_map(
        per_device,
        mesh=mesh,
        in_specs=placed,
        out_specs=P("fs", ("sp", "tp"), None),
        check_vma=False,
    )
```

```python
import jax
import jax.numpy as jnp
from jax import lax
from jax.experimental import pallas as pl
from jax.experimental.pallas import tpu as pltpu
from jax.sharding import PartitionSpec as P

epsilon = 1e-06
log2e = 1.4426950408889634
bf16, f32 = jnp.bfloat16, jnp.float32
vmem = pl.BlockSpec(memory_space=pltpu.VMEM)
smem = pl.BlockSpec(memory_space=pltpu.SMEM)
rows_by_rows = (((1,), (1,)), ((), ()))


def struct(shape, kind):
    return jax.ShapeDtypeStruct(shape, kind)


def dot(a, b):
    return jnp.dot(a, b, preferred_element_type=f32)


def from_everyone(x, axis):
    copies = jnp.broadcast_to(x, (lax.axis_size(axis), *x.shape))
    return lax.all_to_all(copies, axis, split_axis=0, concat_axis=0, tiled=True)


def side_by_side_kernel(*refs):
    at = 0
    for ref in refs[:-1]:
        refs[-1][:, at : at + ref.shape[1]] = ref[...]
        at += ref.shape[1]


def side_by_side(*arrays):
    columns = sum(a.shape[1] for a in arrays)
    return pl.pallas_call(
        side_by_side_kernel,
        out_shape=struct((arrays[0].shape[0], columns), arrays[0].dtype),
        in_specs=[vmem] * len(arrays),
        out_specs=vmem,
        name="side_by_side",
    )(*arrays)


def start_rows(w_ref, first, count, out_ref, sems):
    copies = []
    for y in range(w_ref.shape[0]):
        copies.append(
            pltpu.make_async_copy(
                w_ref.at[y, :, :, pl.ds(first, count)], out_ref.at[:, y], sems.at[y]
            )
        )
        copies[-1].start()
    return copies


def wait_rows(copies, out_ref):
    for copy in copies:
        copy.wait()
    sp, fs, piece, n = out_ref.shape
    return out_ref[...].reshape(sp * fs * piece, n)


def twice(gain_ref):
    return jnp.concatenate([gain_ref[...], gain_ref[...]], axis=1)


def halves_normed(x, gain):
    half = x.shape[1] // 2
    low = lax.broadcasted_iota(jnp.int32, x.shape, 1) < half
    squares = x * x
    zero = jnp.zeros_like(squares)
    one = jnp.sum(jnp.where(low, squares, zero), axis=1, keepdims=True) / half
    two = jnp.sum(jnp.where(low, zero, squares), axis=1, keepdims=True) / half
    return x * jnp.where(low, lax.rsqrt(one + epsilon), lax.rsqrt(two + epsilon)) * gain


def norm_kernel(x_ref, gain_ref, normed_ref, wide_ref, narrow_ref, in_sems, out_sems):
    blocks, tok, feat = x_ref.shape
    arrivals = [
        pltpu.make_async_copy(x_ref.at[b], wide_ref.at[b], in_sems.at[b]) for b in range(blocks)
    ]
    for copy in arrivals:
        copy.start()
    squares = jnp.zeros((tok, feat), f32)
    for b in range(blocks):
        arrivals[b].wait()
        x = wide_ref[b].astype(f32)
        squares = squares + x * x
    mean = jnp.sum(squares, axis=1, keepdims=True) / (blocks * feat)
    scale = lax.rsqrt(mean + epsilon)
    leaving = []
    for b in range(blocks):
        columns = pl.ds(b * feat, feat)
        narrow_ref[:, columns] = (
            wide_ref[b].astype(f32) * scale * gain_ref[:, columns]
        ).astype(bf16)
        leaving.append(
            pltpu.make_async_copy(
                narrow_ref.at[:, columns], normed_ref.at[:, columns], out_sems.at[b]
            )
        )
        leaving[-1].start()
    for copy in leaving:
        copy.wait()


def key_value_kernel(x_ref, w_ref, key_gain_ref, kv_ref, rows_ref, sems):
    both = dot(x_ref[...], wait_rows(start_rows(w_ref, 0, w_ref.shape[3], rows_ref, sems), rows_ref))
    width = 2 * key_gain_ref.shape[1]
    kv_ref[:, :width] = halves_normed(both[:, :width], twice(key_gain_ref)).astype(bf16)
    kv_ref[:, width:] = both[:, width:].astype(bf16)


def query_kernel(
    x_ref, edge_ref, w_ref, gain_ref, all_taps_ref, me_ref, q_ref, filtered_ref,
    rows_ref, signal_ref, sems,
):
    tok, channels = filtered_ref.shape
    width = 2 * gain_ref.shape[1]
    weights = wait_rows(start_rows(w_ref, 0, w_ref.shape[3], rows_ref, sems), rows_ref)
    x = x_ref[...]
    q_ref[...] = halves_normed(dot(x, weights[:, :width]), twice(gain_ref)).astype(bf16)

    def signal_of(rows):
        both = dot(rows, weights[:, width:])
        return (both[:, :channels] * both[:, channels:]).astype(bf16).astype(f32)

    signal = signal_of(x)
    side = signal_of(edge_ref[...])
    signal_ref[8 : tok + 8, :] = signal
    signal_ref[7:8, :] = side[0:1]
    signal_ref[tok + 8 : tok + 9, :] = side[8:9]
    taps = all_taps_ref[:, pl.ds(pl.multiple_of(me_ref[0] * channels, channels), channels)]
    filtered_ref[...] = (
        taps[0:1, :] * signal_ref[7 : tok + 7, :]
        + taps[1:2, :] * signal
        + taps[2:3, :] * signal_ref[9 : tok + 9, :]
    )


def conv_kernel(x_ref, filtered_ref, w_ref, hidden_ref, rows_ref, sems):
    copies = start_rows(w_ref, 0, filtered_ref.shape[1], rows_ref, sems)
    post = dot(x_ref[...], wait_rows(copies, rows_ref)).astype(bf16).astype(f32)
    hidden_ref[...] = (post * filtered_ref[...]).astype(bf16)


def attention_kernel(
    q_ref, kv_ref, lam_ref, gain_ref, conv_ref, out_w_ref, me_ref, mine_ref, theirs_ref,
    acc_ref, both_ref, one_ref, two_ref, all_ref, conv_in_ref, rows_ref, sems, w_sems,
):
    tok, width = q_ref.shape
    half = width // 2
    length = kv_ref.shape[0]
    block = one_ref.shape[0]
    steps = length // block
    me = me_ref[0]
    early = 3 * block

    def arrival(start, size, k):
        rows = pl.ds(start, size)
        return pltpu.make_async_copy(kv_ref.at[rows], all_ref.at[rows], sems.at[k])

    head, tail = arrival(0, early, 0), arrival(early, length - early, 1)
    head.start()
    tail.start()
    channels = conv_ref.shape[1]
    conv_copy = pltpu.make_async_copy(conv_ref, conv_in_ref, sems.at[2])
    conv_copy.start()
    copies = start_rows(out_w_ref, channels, rows_ref.shape[3], rows_ref, w_sems)
    q = q_ref[...].astype(f32) * (log2e * half ** (-0.5))
    high = q.astype(bf16)
    low = (q - high.astype(f32)).astype(bf16)
    lane = lax.broadcasted_iota(jnp.int32, q.shape, 1)
    zero = jnp.zeros_like(high)
    both = jnp.concatenate(
        [
            jnp.concatenate([jnp.where(mask, high, zero), jnp.where(mask, low, zero)], axis=1)
            for mask in (lane < half, lane >= half)
        ],
        axis=0,
    )
    both_ref[...] = jnp.transpose(both.astype(f32)).astype(bf16)
    acc_ref[...] = jnp.zeros_like(acc_ref)

    def rows_of(i):
        return pl.ds(pl.multiple_of(i * block, block), block)

    span = 256
    parts = [slice(n, n + span) for n in range(0, 2 * tok, span)]

    def scores_of(i, s_ref, part):
        key = all_ref[rows_of(i), :width]
        scores = dot(jnp.concatenate([key, key], axis=1), both_ref[:, part])
        s_ref[:, part] = scores
        return jnp.max(scores, axis=0, keepdims=True)

    def take(i, s_ref, part, top, peak, total):
        new_peak = jnp.maximum(peak, top)
        factor = jnp.exp2(peak - new_peak)
        expo = jnp.exp2(s_ref[:, part] - new_peak)
        total = total * factor + jnp.sum(expo, axis=0, keepdims=True)
        acc_ref[:, part] = acc_ref[:, part] * factor + lax.dot_general(
            all_ref[rows_of(i), width:], expo.astype(bf16), (((0,), (0,)), ((), ())),
            preferred_element_type=f32,
        )
        return new_peak, total

    def stage(i, state, here, there):
        result = []
        for part, (top, peak, total) in zip(parts, state):
            next_top = scores_of(jnp.minimum(i + 1, steps - 1), there, part)
            result.append((next_top, *take(i, here, part, top, peak, total)))
        return result

    def step(j, state):
        @pl.when(j == 1)
        def _():
            tail.wait()

        state = stage(2 * j, state, one_ref, two_ref)
        return stage(2 * j + 1, state, two_ref, one_ref)

    head.wait()
    zeros = jnp.zeros((1, span), f32)
    state = [(scores_of(0, one_ref, part), zeros - 1e30, zeros) for part in parts]
    state = lax.fori_loop(0, steps // 2, step, state)
    total = jnp.concatenate([total for _, _, total in state], axis=1)
    mapped = acc_ref[...] / total
    out = mapped[:, :tok] - lam_ref[me] * mapped[:, tok:]
    scaled = out * lax.rsqrt(jnp.mean(out * out, axis=0, keepdims=True) + epsilon)
    hidden = (jnp.transpose(scaled) * gain_ref[...]).astype(bf16)
    weights = wait_rows(copies, rows_ref)
    conv_copy.wait()
    part = lax.dot_general(
        jnp.concatenate([conv_in_ref[...], hidden], axis=1), weights, rows_by_rows,
        preferred_element_type=f32,
    )
    chips, rows, _ = mine_ref.shape
    first_core = (me & 1) == 0
    for chip in range(chips):
        one = part[2 * chip * rows : (2 * chip + 1) * rows]
        two = part[(2 * chip + 1) * rows : (2 * chip + 2) * rows]
        mine_ref[chip] = jnp.where(first_core, one, two).astype(bf16)
        theirs_ref[chip] = jnp.where(first_core, two, one).astype(bf16)


def per_device(
    inputs,
    norm_gain,
    query_weight,
    key_weight,
    value_weight,
    query_gain,
    key_gain,
    mix_lambda,
    head_gain,
    post_gate_weight,
    pre_gate_weight,
    inner_weight,
    conv_taps,
    attn_out_weight,
    conv_out_weight,
):
    tokens = inputs[0]
    tok, feat = tokens.shape
    sp, tp = lax.axis_size("sp"), lax.axis_size("tp")
    total_feat = tp * feat
    width = key_weight.shape[1]
    vsize = head_gain.shape[0]
    channels = post_gate_weight.shape[1]
    piece = key_weight.shape[0]
    out_rows = tok // tp
    chips = tp // 2
    me = lax.axis_index("tp").astype(jnp.int32).reshape(1)
    key_gain, query_gain = key_gain.reshape(1, -1), query_gain.reshape(1, -1)
    in_hbm = pl.BlockSpec(memory_space=pl.ANY)

    def by_rows(tiles):
        return tiles.reshape(tiles.shape[0], sp, piece, tiles.shape[2])

    def ordered(columns):
        return pltpu.VMEM((sp, total_feat // (sp * piece), piece, columns), bf16)

    def sems(count):
        return pltpu.SemaphoreType.DMA((count,))

    fs = lax.axis_size("fs")

    whole = lax.all_gather(tokens, "tp", axis=0, tiled=False)
    first = side_by_side(
        key_weight, value_weight, query_weight, pre_gate_weight, inner_weight
    )
    first = lax.all_gather(first, "sp", axis=0, tiled=True)
    kv_weight = from_everyone(first[:, : width + vsize], "fs")
    normed = pl.pallas_call(
        norm_kernel,
        out_shape=struct((tok, total_feat), bf16),
        in_specs=[in_hbm, vmem],
        out_specs=in_hbm,
        scratch_shapes=[
            pltpu.VMEM((tp, tok, feat), bf16),
            pltpu.VMEM((tok, total_feat), bf16),
            sems(tp),
            sems(tp),
        ],
        cost_estimate=pl.CostEstimate(flops=2 * 10**9, bytes_accessed=2**22, transcendentals=0),
        name="norm",
    )(whole, norm_gain.reshape(1, total_feat))
    kv = pl.pallas_call(
        key_value_kernel,
        out_shape=struct((tok, width + vsize), bf16),
        in_specs=[vmem, in_hbm, vmem],
        out_specs=vmem,
        scratch_shapes=[ordered(width + vsize), sems(fs)],
        name="key_value",
    )(normed, by_rows(kv_weight), key_gain)
    kv_all = lax.all_gather(kv, "sp", axis=0, tiled=True)

    up = [(i, i + 1) for i in range(sp - 1)]
    before = lax.ppermute(normed[tok - 8 :], "sp", up)
    after = lax.ppermute(normed[:8], "sp", [(j, i) for i, j in up])
    edge = jnp.concatenate([before[7:], before[:7], after], axis=0)

    one, _ = lax.optimization_barrier((first[:, width + vsize :], kv_weight))
    one = from_everyone(one, "fs")
    second = side_by_side(post_gate_weight, conv_out_weight, attn_out_weight)
    second, _ = lax.optimization_barrier((second, kv))
    second = lax.all_gather(second, "sp", axis=0, tiled=True)
    query, filtered = pl.pallas_call(
        query_kernel,
        out_shape=(struct((tok, width), bf16), struct((tok, channels), f32)),
        in_specs=[vmem, vmem, in_hbm, vmem, vmem, smem],
        out_specs=(vmem, vmem),
        scratch_shapes=[
            ordered(width + 2 * channels),
            pltpu.VMEM((tok + 16, channels), f32),
            sems(fs),
        ],
        name="query",
    )(normed, edge, by_rows(one), query_gain, conv_taps, me)

    two = by_rows(from_everyone(second, "fs"))
    conv_hidden = pl.pallas_call(
        conv_kernel,
        out_shape=struct((tok, channels), bf16),
        in_specs=[vmem, vmem, in_hbm],
        out_specs=vmem,
        scratch_shapes=[ordered(channels), sems(fs)],
        name="conv",
    )(normed, filtered, two)

    mine, theirs = pl.pallas_call(
        attention_kernel,
        out_shape=(struct((chips, out_rows, total_feat), bf16),) * 2,
        in_specs=[vmem, in_hbm, smem, vmem, in_hbm, in_hbm, smem],
        out_specs=(vmem, vmem),
        scratch_shapes=[
            pltpu.VMEM((vsize, 2 * tok), f32),
            pltpu.VMEM((2 * width, 2 * tok), bf16),
        ]
        + [pltpu.VMEM((512, 2 * tok), f32)] * 2
        + [pltpu.VMEM(kv_all.shape, bf16), pltpu.VMEM((tok, channels), bf16)]
        + [ordered(channels + vsize), sems(3), sems(fs)],
        cost_estimate=pl.CostEstimate(
            flops=8 * tok * kv_all.shape[0] * vsize, bytes_accessed=kv_all.size * 2, transcendentals=0
        ),
        name="attention",
    )(query, kv_all, mix_lambda, head_gain.reshape(1, vsize), conv_hidden, two, me)
    theirs = lax.ppermute(theirs, "tp", [(i, i ^ 1) for i in range(tp)])
    part = (mine.astype(f32) + theirs.astype(f32)).astype(bf16)
    same_core = [list(range(c, tp, 2)) for c in range(2)]
    arrived = lax.all_to_all(
        part, "tp", split_axis=0, concat_axis=0, tiled=True, axis_index_groups=same_core
    )
    return jnp.sum(arrived.astype(f32), axis=0).astype(bf16)[None]


def solution(mesh):
    weight = P(("sp", "fs"), "tp")
    placed = (P("fs", "sp", "tp"), P(), weight, weight, weight, P(), P(), P(), P())
    placed = placed + (weight, weight, weight, P(), weight, weight)
    return jax.shard_map(
        per_device,
        mesh=mesh,
        in_specs=placed,
        out_specs=P("fs", ("sp", "tp"), None),
        check_vma=False,
    )
```

```python
import jax
import jax.numpy as jnp
from jax import lax
from jax.experimental import pallas as pl
from jax.experimental.pallas import tpu as pltpu
from jax.sharding import PartitionSpec as P

epsilon = 1e-06
log2e = 1.4426950408889634
bf16, f32 = jnp.bfloat16, jnp.float32
vmem = pl.BlockSpec(memory_space=pltpu.VMEM)
smem = pl.BlockSpec(memory_space=pltpu.SMEM)
rows_by_rows = (((1,), (1,)), ((), ()))


def struct(shape, kind):
    return jax.ShapeDtypeStruct(shape, kind)


def dot(a, b):
    return jnp.dot(a, b, preferred_element_type=f32)


def from_everyone(x, axis):
    copies = jnp.broadcast_to(x, (lax.axis_size(axis), *x.shape))
    return lax.all_to_all(copies, axis, split_axis=0, concat_axis=0, tiled=True)


def side_by_side_kernel(*refs):
    at = 0
    for ref in refs[:-1]:
        refs[-1][:, at : at + ref.shape[1]] = ref[...]
        at += ref.shape[1]
    if at < refs[-1].shape[1]:
        rows, columns = refs[-1].shape
        refs[-1][:, at:] = jnp.zeros((rows, columns - at), refs[-1].dtype)


def side_by_side(*arrays, least=0):
    columns = max(least, sum(a.shape[1] for a in arrays))
    return pl.pallas_call(
        side_by_side_kernel,
        out_shape=struct((arrays[0].shape[0], columns), arrays[0].dtype),
        in_specs=[vmem] * len(arrays),
        out_specs=vmem,
        name="side_by_side",
    )(*arrays)


def start_rows(w_ref, first, count, out_ref, sems, parity=None):
    copies = []
    columns = pl.ds(first, count)
    for y in range(w_ref.shape[0]):
        if parity is None:
            pairs = [(w_ref.at[y, :, :, columns], out_ref.at[:, y])]
        else:
            pairs = [
                (w_ref.at[y, s, :, :, columns], out_ref.at[:, parity ^ s, y]) for s in range(2)
            ]
        for source, target in pairs:
            copies.append(pltpu.make_async_copy(source, target, sems.at[len(copies)]))
            copies[-1].start()
    return copies


def wait_rows(copies, out_ref):
    for copy in copies:
        copy.wait()
    n = out_ref.shape[-1]
    rows = out_ref[...]
    return rows.reshape(rows.size // n, n)


def load_normed(own_ref, pair_ref, gain_ref, me, wide_ref, narrow_ref, sems):
    blocks, tok, feat = wide_ref.shape
    chips = blocks // 2
    arrivals = []
    for d in range(chips):
        for k, ref in enumerate((own_ref, pair_ref)):
            block = 2 * (((me >> 1) - d) & (chips - 1)) + ((me & 1) ^ k)
            arrivals.append(
                pltpu.make_async_copy(ref.at[d], wide_ref.at[block], sems.at[2 * d + k])
            )
            arrivals[-1].start()
    for copy in arrivals:
        copy.wait()
    squares = jnp.zeros((tok, feat), f32)
    for b in range(blocks):
        x = wide_ref[b].astype(f32)
        squares = squares + x * x
    scale = lax.rsqrt(jnp.sum(squares, axis=1, keepdims=True) / (blocks * feat) + epsilon)
    for b in range(blocks):
        columns = pl.ds(b * feat, feat)
        narrow_ref[:, columns] = (
            wide_ref[b].astype(f32) * scale * gain_ref[:, columns]
        ).astype(bf16)


def twice(gain_ref):
    return jnp.concatenate([gain_ref[...], gain_ref[...]], axis=1)


def halves_normed(x, gain):
    half = x.shape[1] // 2
    low = lax.broadcasted_iota(jnp.int32, x.shape, 1) < half
    squares = x * x
    zero = jnp.zeros_like(squares)
    one = jnp.sum(jnp.where(low, squares, zero), axis=1, keepdims=True) / half
    two = jnp.sum(jnp.where(low, zero, squares), axis=1, keepdims=True) / half
    return x * jnp.where(low, lax.rsqrt(one + epsilon), lax.rsqrt(two + epsilon)) * gain


def key_value_kernel(
    own_ref, pair_ref, gain_ref, w_ref, key_gain_ref, me_ref, kv_ref,
    wide_ref, narrow_ref, rows_ref, in_sems, w_sems,
):
    copies = start_rows(w_ref, 0, w_ref.shape[3], rows_ref, w_sems)
    load_normed(own_ref, pair_ref, gain_ref, me_ref[0], wide_ref, narrow_ref, in_sems)
    both = dot(narrow_ref[...], wait_rows(copies, rows_ref))
    width = 2 * key_gain_ref.shape[1]
    kv_ref[:, :width] = halves_normed(both[:, :width], twice(key_gain_ref)).astype(bf16)
    kv_ref[:, width:] = both[:, width:].astype(bf16)


def query_kernel(
    own_ref, pair_ref, norm_gain_ref, w_ref, gain_ref, me_ref, q_ref, signal_ref, normed_ref,
    wide_ref, narrow_ref, rows_ref, in_sems, w_sems, out_sem,
):
    channels = signal_ref.shape[1]
    width = 2 * gain_ref.shape[1]
    copies = start_rows(w_ref, 0, w_ref.shape[4], rows_ref, w_sems, me_ref[1])
    load_normed(own_ref, pair_ref, norm_gain_ref, me_ref[0], wide_ref, narrow_ref, in_sems)
    leaving = pltpu.make_async_copy(narrow_ref, normed_ref, out_sem.at[0])
    leaving.start()
    weights = wait_rows(copies, rows_ref)
    x = narrow_ref[...]
    q_ref[...] = halves_normed(dot(x, weights[:, :width]), twice(gain_ref)).astype(bf16)
    both = dot(x, weights[:, width:])
    signal_ref[...] = (both[:, :channels] * both[:, channels:]).astype(bf16)
    leaving.wait()


def conv_kernel(
    x_ref, signal_ref, before_ref, after_ref, w_ref, all_taps_ref, me_ref, hidden_ref,
    wide_ref, rows_ref, sems,
):
    tok, channels = hidden_ref.shape
    copies = start_rows(w_ref, 0, channels, rows_ref, sems, me_ref[1])
    signal = signal_ref[...].astype(f32)
    wide_ref[8 : tok + 8, :] = signal
    wide_ref[7:8, :] = before_ref[...].astype(f32)[7:8]
    wide_ref[tok + 8 : tok + 9, :] = after_ref[...].astype(f32)[0:1]
    taps = all_taps_ref[:, pl.ds(pl.multiple_of(me_ref[0] * channels, channels), channels)]
    filtered = (
        taps[0:1, :] * wide_ref[7 : tok + 7, :]
        + taps[1:2, :] * signal
        + taps[2:3, :] * wide_ref[9 : tok + 9, :]
    )
    post = dot(x_ref[...], wait_rows(copies, rows_ref)).astype(bf16).astype(f32)
    hidden_ref[...] = (post * filtered).astype(bf16)


def attention_kernel(
    q_ref, kv_ref, lam_ref, gain_ref, conv_ref, out_w_ref, me_ref, mine_ref, theirs_ref,
    acc_ref, both_ref, one_ref, two_ref, all_ref, conv_in_ref, rows_ref, sems, w_sems,
):
    tok, width = q_ref.shape
    half = width // 2
    length = kv_ref.shape[0]
    block = one_ref.shape[0]
    steps = length // block
    me = me_ref[0]
    early = 3 * block

    def arrival(start, size, k):
        rows = pl.ds(start, size)
        return pltpu.make_async_copy(kv_ref.at[rows], all_ref.at[rows], sems.at[k])

    head, tail = arrival(0, early, 0), arrival(early, length - early, 1)
    head.start()
    tail.start()
    channels = conv_ref.shape[1]
    conv_copy = pltpu.make_async_copy(conv_ref, conv_in_ref, sems.at[2])
    conv_copy.start()
    copies = start_rows(out_w_ref, channels, rows_ref.shape[4], rows_ref, w_sems, me_ref[1])
    q = q_ref[...].astype(f32) * (log2e * half ** (-0.5))
    high = q.astype(bf16)
    low = (q - high.astype(f32)).astype(bf16)
    lane = lax.broadcasted_iota(jnp.int32, q.shape, 1)
    zero = jnp.zeros_like(high)
    both = jnp.concatenate(
        [
            jnp.concatenate([jnp.where(mask, high, zero), jnp.where(mask, low, zero)], axis=1)
            for mask in (lane < half, lane >= half)
        ],
        axis=0,
    )
    both_ref[...] = jnp.transpose(both.astype(f32)).astype(bf16)
    acc_ref[...] = jnp.zeros_like(acc_ref)

    def rows_of(i):
        return pl.ds(pl.multiple_of(i * block, block), block)

    span = 256
    parts = [slice(n, n + span) for n in range(0, 2 * tok, span)]

    def scores_of(i, s_ref, part):
        key = all_ref[rows_of(i), :width]
        scores = dot(jnp.concatenate([key, key], axis=1), both_ref[:, part])
        s_ref[:, part] = scores
        return jnp.max(scores, axis=0, keepdims=True)

    def take(i, s_ref, part, top, peak, total):
        new_peak = jnp.maximum(peak, top)
        factor = jnp.exp2(peak - new_peak)
        expo = jnp.exp2(s_ref[:, part] - new_peak)
        total = total * factor + jnp.sum(expo, axis=0, keepdims=True)
        acc_ref[:, part] = acc_ref[:, part] * factor + lax.dot_general(
            all_ref[rows_of(i), width:], expo.astype(bf16), (((0,), (0,)), ((), ())),
            preferred_element_type=f32,
        )
        return new_peak, total

    def stage(i, state, here, there):
        result = []
        for part, (top, peak, total) in zip(parts, state):
            next_top = scores_of(jnp.minimum(i + 1, steps - 1), there, part)
            result.append((next_top, *take(i, here, part, top, peak, total)))
        return result

    def step(j, state):
        @pl.when(j == 1)
        def _():
            tail.wait()

        state = stage(2 * j, state, one_ref, two_ref)
        return stage(2 * j + 1, state, two_ref, one_ref)

    head.wait()
    zeros = jnp.zeros((1, span), f32)
    state = [(scores_of(0, one_ref, part), zeros - 1e30, zeros) for part in parts]
    state = lax.fori_loop(0, steps // 2, step, state)
    total = jnp.concatenate([total for _, _, total in state], axis=1)
    mapped = acc_ref[...] / total
    out = mapped[:, :tok] - lam_ref[me] * mapped[:, tok:]
    scaled = out * lax.rsqrt(jnp.mean(out * out, axis=0, keepdims=True) + epsilon)
    hidden = (jnp.transpose(scaled) * gain_ref[...]).astype(bf16)
    weights = wait_rows(copies, rows_ref)
    conv_copy.wait()
    part = lax.dot_general(
        jnp.concatenate([conv_in_ref[...], hidden], axis=1), weights, rows_by_rows,
        preferred_element_type=f32,
    )
    chips, rows, _ = mine_ref.shape
    first_core = (me & 1) == 0
    for chip in range(chips):
        one = part[2 * chip * rows : (2 * chip + 1) * rows]
        two = part[(2 * chip + 1) * rows : (2 * chip + 2) * rows]
        mine_ref[chip] = jnp.where(first_core, one, two).astype(bf16)
        theirs_ref[chip] = jnp.where(first_core, two, one).astype(bf16)


def per_device(
    inputs,
    norm_gain,
    query_weight,
    key_weight,
    value_weight,
    query_gain,
    key_gain,
    mix_lambda,
    head_gain,
    post_gate_weight,
    pre_gate_weight,
    inner_weight,
    conv_taps,
    attn_out_weight,
    conv_out_weight,
):
    tokens = inputs[0]
    tok, feat = tokens.shape
    sp, tp = lax.axis_size("sp"), lax.axis_size("tp")
    total_feat = tp * feat
    width = key_weight.shape[1]
    vsize = head_gain.shape[0]
    channels = post_gate_weight.shape[1]
    piece = key_weight.shape[0]
    out_rows = tok // tp
    chips = tp // 2
    me = jnp.stack([lax.axis_index("tp"), lax.axis_index("sp") & 1]).astype(jnp.int32)
    key_gain, query_gain = key_gain.reshape(1, -1), query_gain.reshape(1, -1)
    in_hbm = pl.BlockSpec(memory_space=pl.ANY)

    fs = lax.axis_size("fs")

    def ordered(columns):
        return pltpu.VMEM((sp // 2, 2, fs, piece, columns), bf16)

    def sems(count):
        return pltpu.SemaphoreType.DMA((count,))

    def shifted(x, d):
        return lax.ppermute(x, "tp", [(i, (i + 2 * d) % tp) for i in range(tp)])

    def to_pair(x):
        return lax.ppermute(x, "tp", [(i, i ^ 1) for i in range(tp)])

    def to_neighbour(x):
        return lax.ppermute(x, "sp", [(i, i ^ 1) for i in range(sp)])

    rest = side_by_side(
        query_weight, pre_gate_weight, inner_weight,
        post_gate_weight, conv_out_weight, attn_out_weight, least=2048,
    )
    parities = [list(range(k, sp, 2)) for k in range(2)]
    rest = lax.all_gather(rest, "sp", axis=0, tiled=True, axis_index_groups=parities)
    kv_weight = from_everyone(side_by_side(key_weight, value_weight), "sp")
    own = jnp.stack([tokens] + [shifted(tokens, d) for d in range(1, chips)])
    pair = to_pair(own)
    kv_weight = from_everyone(kv_weight.reshape(sp * piece, width + vsize), "fs")
    row_gain = norm_gain.reshape(1, total_feat)
    kv = pl.pallas_call(
        key_value_kernel,
        out_shape=struct((tok, width + vsize), bf16),
        in_specs=[in_hbm, in_hbm, vmem, in_hbm, vmem, smem],
        out_specs=vmem,
        scratch_shapes=[
            pltpu.VMEM((tp, tok, feat), bf16),
            pltpu.VMEM((tok, total_feat), bf16),
            pltpu.VMEM((sp, fs, piece, width + vsize), bf16),
            sems(tp),
            sems(fs),
        ],
        name="key_value",
    )(own, pair, row_gain, kv_weight.reshape(fs, sp, piece, -1), key_gain, me)
    kv_all = lax.all_gather(kv, "sp", axis=0, tiled=True)

    rest, _ = lax.optimization_barrier((rest, kv))
    split = width + 2 * channels

    def both_parities(columns):
        return jnp.stack([columns, to_neighbour(columns)]).reshape(sp * piece, -1)

    one, two = both_parities(rest[:, :split]), both_parities(rest[:, split : 2 * split])
    one = from_everyone(one, "fs")
    two, _ = lax.optimization_barrier((two, one))
    two = from_everyone(two, "fs")
    query, signal, normed = pl.pallas_call(
        query_kernel,
        out_shape=(
            struct((tok, width), bf16), struct((tok, channels), bf16), struct((tok, total_feat), bf16)
        ),
        in_specs=[in_hbm, in_hbm, vmem, in_hbm, vmem, smem],
        out_specs=(vmem, vmem, in_hbm),
        scratch_shapes=[
            pltpu.VMEM((tp, tok, feat), bf16),
            pltpu.VMEM((tok, total_feat), bf16),
            ordered(split),
            sems(tp),
            sems(2 * fs),
            sems(1),
        ],
        name="query",
    )(own, pair, row_gain, one.reshape(fs, 2, sp // 2, piece, -1), query_gain, me)
    up = [(i, i + 1) for i in range(sp - 1)]
    before = lax.ppermute(signal[tok - 8 :], "sp", up)
    after = lax.ppermute(signal[:8], "sp", [(j, i) for i, j in up])
    two = two.reshape(fs, 2, sp // 2, piece, -1)
    conv_hidden = pl.pallas_call(
        conv_kernel,
        out_shape=struct((tok, channels), bf16),
        in_specs=[vmem, vmem, vmem, vmem, in_hbm, vmem, smem],
        out_specs=vmem,
        scratch_shapes=[pltpu.VMEM((tok + 16, channels), f32), ordered(channels), sems(2 * fs)],
        name="conv",
    )(normed, signal, before, after, two, conv_taps, me)

    mine, theirs = pl.pallas_call(
        attention_kernel,
        out_shape=(struct((chips, out_rows, total_feat), bf16),) * 2,
        in_specs=[vmem, in_hbm, smem, vmem, in_hbm, in_hbm, smem],
        out_specs=(vmem, vmem),
        scratch_shapes=[
            pltpu.VMEM((vsize, 2 * tok), f32),
            pltpu.VMEM((2 * width, 2 * tok), bf16),
        ]
        + [pltpu.VMEM((512, 2 * tok), f32)] * 2
        + [pltpu.VMEM(kv_all.shape, bf16), pltpu.VMEM((tok, channels), bf16)]
        + [ordered(channels + vsize), sems(3), sems(2 * fs)],
        cost_estimate=pl.CostEstimate(
            flops=8 * tok * kv_all.shape[0] * vsize, bytes_accessed=kv_all.size * 2, transcendentals=0
        ),
        name="attention",
    )(query, kv_all, mix_lambda, head_gain.reshape(1, vsize), conv_hidden, two, me)
    theirs = to_pair(theirs)
    part = (mine.astype(f32) + theirs.astype(f32)).astype(bf16)
    same_core = [list(range(c, tp, 2)) for c in range(2)]
    arrived = lax.all_to_all(
        part, "tp", split_axis=0, concat_axis=0, tiled=True, axis_index_groups=same_core
    )
    return jnp.sum(arrived.astype(f32), axis=0).astype(bf16)[None]


def solution(mesh):
    weight = P(("sp", "fs"), "tp")
    placed = (P("fs", "sp", "tp"), P(), weight, weight, weight, P(), P(), P(), P())
    placed = placed + (weight, weight, weight, P(), weight, weight)
    return jax.shard_map(
        per_device,
        mesh=mesh,
        in_specs=placed,
        out_specs=P("fs", ("sp", "tp"), None),
        check_vma=False,
    )
```

```python
import jax
import jax.numpy as jnp
from jax import lax
from jax.experimental import pallas as pl
from jax.experimental.pallas import tpu as pltpu
from jax.sharding import PartitionSpec as P

epsilon = 1e-06
log2e = 1.4426950408889634
bf16, f32 = jnp.bfloat16, jnp.float32
vmem = pl.BlockSpec(memory_space=pltpu.VMEM)
smem = pl.BlockSpec(memory_space=pltpu.SMEM)
rows_by_rows = (((1,), (1,)), ((), ()))


def struct(shape, kind):
    return jax.ShapeDtypeStruct(shape, kind)


def dot(a, b):
    return jnp.dot(a, b, preferred_element_type=f32)


def copies_of(x, axis):
    return jnp.broadcast_to(x, (lax.axis_size(axis), *x.shape))


def exchanged(x, axis):
    return lax.all_to_all(x, axis, split_axis=0, concat_axis=0, tiled=True)


def from_everyone(x, axis):
    return exchanged(copies_of(x, axis), axis)


def side_by_side_kernel(*refs):
    at = 0
    for ref in refs[:-1]:
        refs[-1][:, at : at + ref.shape[1]] = ref[...]
        at += ref.shape[1]


def side_by_side(*arrays):
    columns = sum(a.shape[1] for a in arrays)
    return pl.pallas_call(
        side_by_side_kernel,
        out_shape=struct((arrays[0].shape[0], columns), arrays[0].dtype),
        in_specs=[vmem] * len(arrays),
        out_specs=vmem,
        name="side_by_side",
    )(*arrays)


def start_rows(w_ref, first, count, out_ref, sems):
    copies = []
    for y in range(w_ref.shape[0]):
        copies.append(
            pltpu.make_async_copy(
                w_ref.at[y, :, :, pl.ds(first, count)], out_ref.at[:, y], sems.at[y]
            )
        )
        copies[-1].start()
    return copies


def wait_rows(copies, out_ref):
    for copy in copies:
        copy.wait()
    sp, fs, piece, n = out_ref.shape
    return out_ref[...].reshape(sp * fs * piece, n)


def twice(gain_ref):
    return jnp.concatenate([gain_ref[...], gain_ref[...]], axis=1)


def halves_normed(x, gain):
    half = x.shape[1] // 2
    low = lax.broadcasted_iota(jnp.int32, x.shape, 1) < half
    squares = x * x
    zero = jnp.zeros_like(squares)
    one = jnp.sum(jnp.where(low, squares, zero), axis=1, keepdims=True) / half
    two = jnp.sum(jnp.where(low, zero, squares), axis=1, keepdims=True) / half
    return x * jnp.where(low, lax.rsqrt(one + epsilon), lax.rsqrt(two + epsilon)) * gain


def key_value_kernel(
    x_ref, gain_ref, w_ref, key_gain_ref, normed_ref, kv_ref,
    wide_ref, narrow_ref, rows_ref, in_sems, w_sems, out_sems,
):
    blocks, tok, feat = x_ref.shape
    arrivals = [
        pltpu.make_async_copy(x_ref.at[b], wide_ref.at[b], in_sems.at[b]) for b in range(blocks)
    ]
    for copy in arrivals:
        copy.start()
    copies = start_rows(w_ref, 0, w_ref.shape[3], rows_ref, w_sems)
    squares = jnp.zeros((tok, feat), f32)
    for b in range(blocks):
        arrivals[b].wait()
        x = wide_ref[b].astype(f32)
        squares = squares + x * x
    mean = jnp.sum(squares, axis=1, keepdims=True) / (blocks * feat)
    scale = lax.rsqrt(mean + epsilon)
    leaving = []
    for b in range(blocks):
        columns = pl.ds(b * feat, feat)
        narrow_ref[:, columns] = (
            wide_ref[b].astype(f32) * scale * gain_ref[:, columns]
        ).astype(bf16)
        leaving.append(
            pltpu.make_async_copy(
                narrow_ref.at[:, columns], normed_ref.at[:, columns], out_sems.at[b]
            )
        )
        leaving[-1].start()
    both = dot(narrow_ref[...], wait_rows(copies, rows_ref))
    width = 2 * key_gain_ref.shape[1]
    kv_ref[:, :width] = halves_normed(both[:, :width], twice(key_gain_ref)).astype(bf16)
    kv_ref[:, width:] = both[:, width:].astype(bf16)
    for copy in leaving:
        copy.wait()


def query_kernel(
    x_ref, edge_ref, w_ref, gain_ref, all_taps_ref, me_ref, q_ref, filtered_ref,
    rows_ref, signal_ref, sems,
):
    tok, channels = filtered_ref.shape
    width = 2 * gain_ref.shape[1]
    weights = wait_rows(start_rows(w_ref, 0, w_ref.shape[3], rows_ref, sems), rows_ref)
    x = x_ref[...]
    q_ref[...] = halves_normed(dot(x, weights[:, :width]), twice(gain_ref)).astype(bf16)

    def signal_of(rows):
        both = dot(rows, weights[:, width:])
        return (both[:, :channels] * both[:, channels:]).astype(bf16).astype(f32)

    signal = signal_of(x)
    side = signal_of(edge_ref[...])
    signal_ref[8 : tok + 8, :] = signal
    signal_ref[7:8, :] = side[0:1]
    signal_ref[tok + 8 : tok + 9, :] = side[8:9]
    taps = all_taps_ref[:, pl.ds(pl.multiple_of(me_ref[0] * channels, channels), channels)]
    filtered_ref[...] = (
        taps[0:1, :] * signal_ref[7 : tok + 7, :]
        + taps[1:2, :] * signal
        + taps[2:3, :] * signal_ref[9 : tok + 9, :]
    )


def conv_kernel(x_ref, filtered_ref, w_ref, hidden_ref, rows_ref, sems):
    copies = start_rows(w_ref, 0, filtered_ref.shape[1], rows_ref, sems)
    post = dot(x_ref[...], wait_rows(copies, rows_ref)).astype(bf16).astype(f32)
    hidden_ref[...] = (post * filtered_ref[...]).astype(bf16)


def attention_kernel(
    q_ref, kv_ref, lam_ref, gain_ref, conv_ref, out_w_ref, me_ref, mine_ref, theirs_ref,
    acc_ref, both_ref, one_ref, two_ref, all_ref, conv_in_ref, rows_ref, out_ref,
    sems, w_sems, out_sems,
):
    tok, width = q_ref.shape
    half = width // 2
    length = kv_ref.shape[0]
    block = one_ref.shape[0]
    steps = length // block
    me = me_ref[0]
    early = 3 * block

    def arrival(start, size, k):
        rows = pl.ds(start, size)
        return pltpu.make_async_copy(kv_ref.at[rows], all_ref.at[rows], sems.at[k])

    head, tail = arrival(0, early, 0), arrival(early, length - early, 1)
    head.start()
    tail.start()
    channels = conv_ref.shape[1]
    conv_copy = pltpu.make_async_copy(conv_ref, conv_in_ref, sems.at[2])
    conv_copy.start()
    copies = start_rows(out_w_ref, channels, rows_ref.shape[3], rows_ref, w_sems)
    q = q_ref[...].astype(f32) * (log2e * half ** (-0.5))
    high = q.astype(bf16)
    low = (q - high.astype(f32)).astype(bf16)
    lane = lax.broadcasted_iota(jnp.int32, q.shape, 1)
    zero = jnp.zeros_like(high)
    both = jnp.concatenate(
        [
            jnp.concatenate([jnp.where(mask, high, zero), jnp.where(mask, low, zero)], axis=1)
            for mask in (lane < half, lane >= half)
        ],
        axis=0,
    )
    both_ref[...] = jnp.transpose(both.astype(f32)).astype(bf16)
    acc_ref[...] = jnp.zeros_like(acc_ref)

    def rows_of(i):
        return pl.ds(pl.multiple_of(i * block, block), block)

    span = 256
    parts = [slice(n, n + span) for n in range(0, 2 * tok, span)]

    def scores_of(i, s_ref, part):
        key = all_ref[rows_of(i), :width]
        scores = dot(jnp.concatenate([key, key], axis=1), both_ref[:, part])
        s_ref[:, part] = scores
        return jnp.max(scores, axis=0, keepdims=True)

    def take(i, s_ref, part, top, peak, total):
        new_peak = jnp.maximum(peak, top)
        factor = jnp.exp2(peak - new_peak)
        expo = jnp.exp2(s_ref[:, part] - new_peak)
        total = total * factor + jnp.sum(expo, axis=0, keepdims=True)
        acc_ref[:, part] = acc_ref[:, part] * factor + lax.dot_general(
            all_ref[rows_of(i), width:], expo.astype(bf16), (((0,), (0,)), ((), ())),
            preferred_element_type=f32,
        )
        return new_peak, total

    def stage(i, state, here, there):
        result = []
        for part, (top, peak, total) in zip(parts, state):
            next_top = scores_of(jnp.minimum(i + 1, steps - 1), there, part)
            result.append((next_top, *take(i, here, part, top, peak, total)))
        return result

    def step(j, state):
        @pl.when(j == 1)
        def _():
            tail.wait()

        state = stage(2 * j, state, one_ref, two_ref)
        return stage(2 * j + 1, state, two_ref, one_ref)

    head.wait()
    zeros = jnp.zeros((1, span), f32)
    state = [(scores_of(0, one_ref, part), zeros - 1e30, zeros) for part in parts]
    state = lax.fori_loop(0, steps // 2, step, state)
    total = jnp.concatenate([total for _, _, total in state], axis=1)
    mapped = acc_ref[...] / total
    out = mapped[:, :tok] - lam_ref[me] * mapped[:, tok:]
    scaled = out * lax.rsqrt(jnp.mean(out * out, axis=0, keepdims=True) + epsilon)
    hidden = (jnp.transpose(scaled) * gain_ref[...]).astype(bf16)
    weights = wait_rows(copies, rows_ref)
    conv_copy.wait()
    rows = jnp.concatenate([conv_in_ref[...], hidden], axis=1)
    chips, count, _ = mine_ref.shape
    first_core = (me & 1) == 0
    leaving = []
    for k, ref in enumerate((theirs_ref, mine_ref)):
        chosen = []
        for chip in range(chips):
            one = rows[2 * chip * count : (2 * chip + 1) * count]
            two = rows[(2 * chip + 1) * count : (2 * chip + 2) * count]
            chosen.append(jnp.where(first_core == (k == 1), one, two))
        part = lax.dot_general(
            jnp.concatenate(chosen, axis=0), weights, rows_by_rows, preferred_element_type=f32
        ).astype(bf16)
        for chip in range(chips):
            out_ref[k, chip] = part[chip * count : (chip + 1) * count]
        leaving.append(pltpu.make_async_copy(out_ref.at[k], ref, out_sems.at[k]))
        leaving[-1].start()
    for copy in leaving:
        copy.wait()


def per_device(
    inputs,
    norm_gain,
    query_weight,
    key_weight,
    value_weight,
    query_gain,
    key_gain,
    mix_lambda,
    head_gain,
    post_gate_weight,
    pre_gate_weight,
    inner_weight,
    conv_taps,
    attn_out_weight,
    conv_out_weight,
):
    tokens = inputs[0]
    tok, feat = tokens.shape
    sp, tp = lax.axis_size("sp"), lax.axis_size("tp")
    total_feat = tp * feat
    width = key_weight.shape[1]
    vsize = head_gain.shape[0]
    channels = post_gate_weight.shape[1]
    piece = key_weight.shape[0]
    out_rows = tok // tp
    chips = tp // 2
    me = lax.axis_index("tp").astype(jnp.int32).reshape(1)
    key_gain, query_gain = key_gain.reshape(1, -1), query_gain.reshape(1, -1)
    in_hbm = pl.BlockSpec(memory_space=pl.ANY)

    def by_rows(tiles):
        return tiles.reshape(tiles.shape[0], sp, piece, tiles.shape[2])

    def ordered(columns):
        return pltpu.VMEM((sp, total_feat // (sp * piece), piece, columns), bf16)

    def sems(count):
        return pltpu.SemaphoreType.DMA((count,))

    fs = lax.axis_size("fs")

    whole = lax.all_gather(tokens, "tp", axis=0, tiled=False)
    first = side_by_side(
        key_weight, value_weight, query_weight, pre_gate_weight, inner_weight
    )
    first = lax.all_gather(first, "sp", axis=0, tiled=True)
    kv_weight = from_everyone(first[:, : width + vsize], "fs")
    normed, kv = pl.pallas_call(
        key_value_kernel,
        out_shape=(struct((tok, total_feat), bf16), struct((tok, width + vsize), bf16)),
        in_specs=[in_hbm, vmem, in_hbm, vmem],
        out_specs=(in_hbm, vmem),
        scratch_shapes=[
            pltpu.VMEM((tp, tok, feat), bf16),
            pltpu.VMEM((tok, total_feat), bf16),
            ordered(width + vsize),
            sems(tp),
            sems(fs),
            sems(tp),
        ],
        name="key_value",
    )(whole, norm_gain.reshape(1, total_feat), by_rows(kv_weight), key_gain)
    kv_all = lax.all_gather(kv, "sp", axis=0, tiled=True)

    up = [(i, i + 1) for i in range(sp - 1)]
    before = lax.ppermute(normed[tok - 8 :], "sp", up)
    after = lax.ppermute(normed[:8], "sp", [(j, i) for i, j in up])
    edge = jnp.concatenate([before[7:], before[:7], after], axis=0)

    one, _ = lax.optimization_barrier((copies_of(first[:, width + vsize :], "fs"), kv_weight))
    one = exchanged(one, "fs")
    second = side_by_side(post_gate_weight, conv_out_weight, attn_out_weight)
    second, _ = lax.optimization_barrier((second, kv))
    second = lax.all_gather(second, "sp", axis=0, tiled=True)
    query, filtered = pl.pallas_call(
        query_kernel,
        out_shape=(struct((tok, width), bf16), struct((tok, channels), f32)),
        in_specs=[vmem, vmem, in_hbm, vmem, vmem, smem],
        out_specs=(vmem, vmem),
        scratch_shapes=[
            ordered(width + 2 * channels),
            pltpu.VMEM((tok + 16, channels), f32),
            sems(fs),
        ],
        name="query",
    )(normed, edge, by_rows(one), query_gain, conv_taps, me)

    two = by_rows(from_everyone(second, "fs"))
    conv_hidden = pl.pallas_call(
        conv_kernel,
        out_shape=struct((tok, channels), bf16),
        in_specs=[vmem, vmem, in_hbm],
        out_specs=vmem,
        scratch_shapes=[ordered(channels), sems(fs)],
        name="conv",
    )(normed, filtered, two)

    mine, theirs = pl.pallas_call(
        attention_kernel,
        out_shape=(struct((chips, out_rows, total_feat), bf16),) * 2,
        in_specs=[vmem, in_hbm, smem, vmem, in_hbm, in_hbm, smem],
        out_specs=(in_hbm, in_hbm),
        scratch_shapes=[
            pltpu.VMEM((vsize, 2 * tok), f32),
            pltpu.VMEM((2 * width, 2 * tok), bf16),
        ]
        + [pltpu.VMEM((512, 2 * tok), f32)] * 2
        + [pltpu.VMEM(kv_all.shape, bf16), pltpu.VMEM((tok, channels), bf16)]
        + [ordered(channels + vsize), pltpu.VMEM((2, chips, out_rows, total_feat), bf16)]
        + [sems(3), sems(fs), sems(2)],
        cost_estimate=pl.CostEstimate(
            flops=8 * tok * kv_all.shape[0] * vsize, bytes_accessed=kv_all.size * 2, transcendentals=0
        ),
        name="attention",
    )(query, kv_all, mix_lambda, head_gain.reshape(1, vsize), conv_hidden, two, me)
    theirs = lax.ppermute(theirs, "tp", [(i, i ^ 1) for i in range(tp)])
    part = (mine.astype(f32) + theirs.astype(f32)).astype(bf16)
    same_core = [list(range(c, tp, 2)) for c in range(2)]
    arrived = lax.all_to_all(
        part, "tp", split_axis=0, concat_axis=0, tiled=True, axis_index_groups=same_core
    )
    return jnp.sum(arrived.astype(f32), axis=0).astype(bf16)[None]


def solution(mesh):
    weight = P(("sp", "fs"), "tp")
    placed = (P("fs", "sp", "tp"), P(), weight, weight, weight, P(), P(), P(), P())
    placed = placed + (weight, weight, weight, P(), weight, weight)
    return jax.shard_map(
        per_device,
        mesh=mesh,
        in_specs=placed,
        out_specs=P("fs", ("sp", "tp"), None),
        check_vma=False,
    )
```

```python
import jax
import jax.numpy as jnp
from jax import lax
from jax.experimental import pallas as pl
from jax.experimental.pallas import tpu as pltpu
from jax.sharding import PartitionSpec as P

epsilon = 1e-06
log2e = 1.4426950408889634
bf16, f32 = jnp.bfloat16, jnp.float32
vmem = pl.BlockSpec(memory_space=pltpu.VMEM)
smem = pl.BlockSpec(memory_space=pltpu.SMEM)
rows_by_rows = (((1,), (1,)), ((), ()))


def struct(shape, kind):
    return jax.ShapeDtypeStruct(shape, kind)


def dot(a, b):
    return jnp.dot(a, b, preferred_element_type=f32)


def copies_of(x, axis):
    return jnp.broadcast_to(x, (lax.axis_size(axis), *x.shape))


def exchanged(x, axis):
    return lax.all_to_all(x, axis, split_axis=0, concat_axis=0, tiled=True)


def from_everyone(x, axis):
    return exchanged(copies_of(x, axis), axis)


def side_by_side_kernel(*refs):
    arrays, out_ref, sems = refs[:-2], refs[-2], refs[-1]
    copies, at = [], 0
    for k, ref in enumerate(arrays):
        columns = pl.ds(at, ref.shape[1])
        copies.append(pltpu.make_async_copy(ref, out_ref.at[:, columns], sems.at[k]))
        copies[-1].start()
        at += ref.shape[1]
    for copy in copies:
        copy.wait()


def side_by_side(*arrays):
    columns = sum(a.shape[1] for a in arrays)
    in_hbm = pl.BlockSpec(memory_space=pl.ANY)
    return pl.pallas_call(
        side_by_side_kernel,
        out_shape=struct((arrays[0].shape[0], columns), arrays[0].dtype),
        in_specs=[in_hbm] * len(arrays),
        out_specs=in_hbm,
        scratch_shapes=[pltpu.SemaphoreType.DMA((len(arrays),))],
        name="side_by_side",
    )(*arrays)


def start_rows(w_ref, first, count, out_ref, sems):
    copies = []
    for y in range(w_ref.shape[0]):
        copies.append(
            pltpu.make_async_copy(
                w_ref.at[y, :, :, pl.ds(first, count)], out_ref.at[:, y], sems.at[y]
            )
        )
        copies[-1].start()
    return copies


def wait_rows(copies, out_ref):
    for copy in copies:
        copy.wait()
    sp, fs, piece, n = out_ref.shape
    return out_ref[...].reshape(sp * fs * piece, n)


def twice(gain_ref):
    return jnp.concatenate([gain_ref[...], gain_ref[...]], axis=1)


def halves_normed(x, gain):
    half = x.shape[1] // 2
    low = lax.broadcasted_iota(jnp.int32, x.shape, 1) < half
    squares = x * x
    zero = jnp.zeros_like(squares)
    one = jnp.sum(jnp.where(low, squares, zero), axis=1, keepdims=True) / half
    two = jnp.sum(jnp.where(low, zero, squares), axis=1, keepdims=True) / half
    return x * jnp.where(low, lax.rsqrt(one + epsilon), lax.rsqrt(two + epsilon)) * gain


def key_value_kernel(
    x_ref, gain_ref, w_ref, key_gain_ref, normed_ref, kv_ref,
    wide_ref, narrow_ref, rows_ref, in_sems, w_sems, out_sems,
):
    blocks, tok, feat = x_ref.shape
    arrivals = [
        pltpu.make_async_copy(x_ref.at[b], wide_ref.at[b], in_sems.at[b]) for b in range(blocks)
    ]
    for copy in arrivals:
        copy.start()
    copies = start_rows(w_ref, 0, w_ref.shape[3], rows_ref, w_sems)
    squares = jnp.zeros((tok, feat), f32)
    for b in range(blocks):
        arrivals[b].wait()
        x = wide_ref[b].astype(f32)
        squares = squares + x * x
    mean = jnp.sum(squares, axis=1, keepdims=True) / (blocks * feat)
    scale = lax.rsqrt(mean + epsilon)
    leaving = []
    for b in range(blocks):
        columns = pl.ds(b * feat, feat)
        narrow_ref[:, columns] = (
            wide_ref[b].astype(f32) * scale * gain_ref[:, columns]
        ).astype(bf16)
        leaving.append(
            pltpu.make_async_copy(
                narrow_ref.at[:, columns], normed_ref.at[:, columns], out_sems.at[b]
            )
        )
        leaving[-1].start()
    both = dot(narrow_ref[...], wait_rows(copies, rows_ref))
    width = 2 * key_gain_ref.shape[1]
    kv_ref[:, :width] = halves_normed(both[:, :width], twice(key_gain_ref)).astype(bf16)
    kv_ref[:, width:] = both[:, width:].astype(bf16)
    for copy in leaving:
        copy.wait()


def query_kernel(
    x_ref, edge_ref, w_ref, gain_ref, all_taps_ref, me_ref, q_ref, filtered_ref,
    rows_ref, signal_ref, sems,
):
    tok, channels = filtered_ref.shape
    width = 2 * gain_ref.shape[1]
    weights = wait_rows(start_rows(w_ref, 0, w_ref.shape[3], rows_ref, sems), rows_ref)
    x = x_ref[...]
    q_ref[...] = halves_normed(dot(x, weights[:, :width]), twice(gain_ref)).astype(bf16)

    def signal_of(rows):
        both = dot(rows, weights[:, width:])
        return (both[:, :channels] * both[:, channels:]).astype(bf16).astype(f32)

    signal = signal_of(x)
    side = signal_of(edge_ref[...])
    signal_ref[8 : tok + 8, :] = signal
    signal_ref[7:8, :] = side[0:1]
    signal_ref[tok + 8 : tok + 9, :] = side[8:9]
    taps = all_taps_ref[:, pl.ds(pl.multiple_of(me_ref[0] * channels, channels), channels)]
    filtered_ref[...] = (
        taps[0:1, :] * signal_ref[7 : tok + 7, :]
        + taps[1:2, :] * signal
        + taps[2:3, :] * signal_ref[9 : tok + 9, :]
    )


def conv_kernel(x_ref, filtered_ref, w_ref, hidden_ref, rows_ref, sems):
    copies = start_rows(w_ref, 0, filtered_ref.shape[1], rows_ref, sems)
    post = dot(x_ref[...], wait_rows(copies, rows_ref)).astype(bf16).astype(f32)
    hidden_ref[...] = (post * filtered_ref[...]).astype(bf16)


def attention_kernel(
    q_ref, kv_ref, lam_ref, gain_ref, conv_ref, out_w_ref, me_ref, mine_ref, theirs_ref,
    acc_ref, both_ref, one_ref, two_ref, all_ref, conv_in_ref, rows_ref, out_ref,
    sems, w_sems, out_sems,
):
    tok, width = q_ref.shape
    half = width // 2
    vsize = gain_ref.shape[1]
    length = kv_ref.shape[0]
    block = one_ref.shape[0]
    steps = length // block
    me = me_ref[0]
    early = 3 * block

    def arrival(start, size, k):
        rows = pl.ds(start, size)
        return pltpu.make_async_copy(kv_ref.at[rows], all_ref.at[rows], sems.at[k])

    head, tail = arrival(0, early, 0), arrival(early, length - early, 1)
    head.start()
    tail.start()
    channels = conv_ref.shape[1]
    conv_copy = pltpu.make_async_copy(conv_ref, conv_in_ref, sems.at[2])
    conv_copy.start()
    copies = start_rows(out_w_ref, channels, rows_ref.shape[3], rows_ref, w_sems)
    q = q_ref[...].astype(f32) * (log2e * half ** (-0.5))
    high = q.astype(bf16)
    low = (q - high.astype(f32)).astype(bf16)
    lane = lax.broadcasted_iota(jnp.int32, q.shape, 1)
    zero = jnp.zeros_like(high)
    both = jnp.concatenate(
        [
            jnp.concatenate([jnp.where(mask, high, zero), jnp.where(mask, low, zero)], axis=1)
            for mask in (lane < half, lane >= half)
        ],
        axis=0,
    )
    both_ref[...] = jnp.transpose(both.astype(f32)).astype(bf16)
    acc_ref[...] = jnp.zeros_like(acc_ref)

    def rows_of(i):
        return pl.ds(pl.multiple_of(i * block, block), block)

    span = 256
    parts = [slice(n, n + span) for n in range(0, 2 * tok, span)]

    def scores_of(i, s_ref, part):
        key = all_ref[rows_of(i), :width]
        scores = dot(jnp.concatenate([key, key], axis=1), both_ref[:, part])
        s_ref[:, part] = scores
        return jnp.max(scores, axis=0, keepdims=True)

    ones = jnp.ones((block, acc_ref.shape[0] - vsize), bf16)

    def take(i, s_ref, part, top, peak):
        new_peak = jnp.maximum(peak, top)
        factor = jnp.exp2(peak - new_peak)
        expo = jnp.exp2(s_ref[:, part] - new_peak)
        acc_ref[:, part] = acc_ref[:, part] * factor + lax.dot_general(
            jnp.concatenate([all_ref[rows_of(i), width:], ones], axis=1), expo.astype(bf16),
            (((0,), (0,)), ((), ())), preferred_element_type=f32,
        )
        return new_peak

    def stage(i, state, here, there):
        result = []
        for part, (top, peak) in zip(parts, state):
            next_top = scores_of(jnp.minimum(i + 1, steps - 1), there, part)
            result.append((next_top, take(i, here, part, top, peak)))
        return result

    def step(j, state):
        @pl.when(j == 1)
        def _():
            tail.wait()

        state = stage(2 * j, state, one_ref, two_ref)
        return stage(2 * j + 1, state, two_ref, one_ref)

    head.wait()
    lowest = jnp.full((1, span), -1e30, f32)
    state = [(scores_of(0, one_ref, part), lowest) for part in parts]
    lax.fori_loop(0, steps // 2, step, state)
    mapped = acc_ref[:vsize] / acc_ref[vsize : vsize + 1]
    out = mapped[:, :tok] - lam_ref[me] * mapped[:, tok:]
    scaled = out * lax.rsqrt(jnp.mean(out * out, axis=0, keepdims=True) + epsilon)
    hidden = (jnp.transpose(scaled) * gain_ref[...]).astype(bf16)
    weights = wait_rows(copies, rows_ref)
    conv_copy.wait()
    rows = jnp.concatenate([conv_in_ref[...], hidden], axis=1)
    chips, count, _ = mine_ref.shape
    first_core = (me & 1) == 0
    leaving = []
    for k, ref in enumerate((theirs_ref, mine_ref)):
        chosen = []
        for chip in range(chips):
            one = rows[2 * chip * count : (2 * chip + 1) * count]
            two = rows[(2 * chip + 1) * count : (2 * chip + 2) * count]
            chosen.append(jnp.where(first_core == (k == 1), one, two))
        part = lax.dot_general(
            jnp.concatenate(chosen, axis=0), weights, rows_by_rows, preferred_element_type=f32
        ).astype(bf16)
        for chip in range(chips):
            out_ref[k, chip] = part[chip * count : (chip + 1) * count]
        leaving.append(pltpu.make_async_copy(out_ref.at[k], ref, out_sems.at[k]))
        leaving[-1].start()
    for copy in leaving:
        copy.wait()


def per_device(
    inputs,
    norm_gain,
    query_weight,
    key_weight,
    value_weight,
    query_gain,
    key_gain,
    mix_lambda,
    head_gain,
    post_gate_weight,
    pre_gate_weight,
    inner_weight,
    conv_taps,
    attn_out_weight,
    conv_out_weight,
):
    tokens = inputs[0]
    tok, feat = tokens.shape
    sp, tp = lax.axis_size("sp"), lax.axis_size("tp")
    total_feat = tp * feat
    width = key_weight.shape[1]
    vsize = head_gain.shape[0]
    channels = post_gate_weight.shape[1]
    piece = key_weight.shape[0]
    out_rows = tok // tp
    chips = tp // 2
    me = lax.axis_index("tp").astype(jnp.int32).reshape(1)
    key_gain, query_gain = key_gain.reshape(1, -1), query_gain.reshape(1, -1)
    in_hbm = pl.BlockSpec(memory_space=pl.ANY)

    def by_rows(tiles):
        return tiles.reshape(tiles.shape[0], sp, piece, tiles.shape[2])

    def ordered(columns):
        return pltpu.VMEM((sp, total_feat // (sp * piece), piece, columns), bf16)

    def sems(count):
        return pltpu.SemaphoreType.DMA((count,))

    fs = lax.axis_size("fs")

    whole = lax.all_gather(tokens, "tp", axis=0, tiled=False)
    first = side_by_side(
        key_weight, value_weight, query_weight, pre_gate_weight, inner_weight
    )
    first = lax.all_gather(first, "sp", axis=0, tiled=True)
    kv_weight = from_everyone(first[:, : width + vsize], "fs")
    normed, kv = pl.pallas_call(
        key_value_kernel,
        out_shape=(struct((tok, total_feat), bf16), struct((tok, width + vsize), bf16)),
        in_specs=[in_hbm, vmem, in_hbm, vmem],
        out_specs=(in_hbm, vmem),
        scratch_shapes=[
            pltpu.VMEM((tp, tok, feat), bf16),
            pltpu.VMEM((tok, total_feat), bf16),
            ordered(width + vsize),
            sems(tp),
            sems(fs),
            sems(tp),
        ],
        name="key_value",
    )(whole, norm_gain.reshape(1, total_feat), by_rows(kv_weight), key_gain)
    kv_all = lax.all_gather(kv, "sp", axis=0, tiled=True)

    up = [(i, i + 1) for i in range(sp - 1)]
    before = lax.ppermute(normed[tok - 8 :], "sp", up)
    after = lax.ppermute(normed[:8], "sp", [(j, i) for i, j in up])
    edge = jnp.concatenate([before[7:], before[:7], after], axis=0)

    one, _ = lax.optimization_barrier((copies_of(first[:, width + vsize :], "fs"), kv_weight))
    one = exchanged(one, "fs")
    second = side_by_side(post_gate_weight, conv_out_weight, attn_out_weight)
    second, _ = lax.optimization_barrier((second, kv))
    second = lax.all_gather(second, "sp", axis=0, tiled=True)
    query, filtered = pl.pallas_call(
        query_kernel,
        out_shape=(struct((tok, width), bf16), struct((tok, channels), f32)),
        in_specs=[vmem, vmem, in_hbm, vmem, vmem, smem],
        out_specs=(vmem, vmem),
        scratch_shapes=[
            ordered(width + 2 * channels),
            pltpu.VMEM((tok + 16, channels), f32),
            sems(fs),
        ],
        name="query",
    )(normed, edge, by_rows(one), query_gain, conv_taps, me)

    two = by_rows(from_everyone(second, "fs"))
    conv_hidden = pl.pallas_call(
        conv_kernel,
        out_shape=struct((tok, channels), bf16),
        in_specs=[vmem, vmem, in_hbm],
        out_specs=vmem,
        scratch_shapes=[ordered(channels), sems(fs)],
        name="conv",
    )(normed, filtered, two)

    mine, theirs = pl.pallas_call(
        attention_kernel,
        out_shape=(struct((chips, out_rows, total_feat), bf16),) * 2,
        in_specs=[vmem, in_hbm, smem, vmem, in_hbm, in_hbm, smem],
        out_specs=(in_hbm, in_hbm),
        scratch_shapes=[
            pltpu.VMEM((vsize + 8, 2 * tok), f32),
            pltpu.VMEM((2 * width, 2 * tok), bf16),
        ]
        + [pltpu.VMEM((512, 2 * tok), f32)] * 2
        + [pltpu.VMEM(kv_all.shape, bf16), pltpu.VMEM((tok, channels), bf16)]
        + [ordered(channels + vsize), pltpu.VMEM((2, chips, out_rows, total_feat), bf16)]
        + [sems(3), sems(fs), sems(2)],
        cost_estimate=pl.CostEstimate(
            flops=8 * tok * kv_all.shape[0] * vsize, bytes_accessed=kv_all.size * 2, transcendentals=0
        ),
        name="attention",
    )(query, kv_all, mix_lambda, head_gain.reshape(1, vsize), conv_hidden, two, me)
    theirs = lax.ppermute(theirs, "tp", [(i, i ^ 1) for i in range(tp)])
    part = (mine.astype(f32) + theirs.astype(f32)).astype(bf16)
    same_core = [list(range(c, tp, 2)) for c in range(2)]
    arrived = lax.all_to_all(
        part, "tp", split_axis=0, concat_axis=0, tiled=True, axis_index_groups=same_core
    )
    return jnp.sum(arrived.astype(f32), axis=0).astype(bf16)[None]


def solution(mesh):
    weight = P(("sp", "fs"), "tp")
    placed = (P("fs", "sp", "tp"), P(), weight, weight, weight, P(), P(), P(), P())
    placed = placed + (weight, weight, weight, P(), weight, weight)
    return jax.shard_map(
        per_device,
        mesh=mesh,
        in_specs=placed,
        out_specs=P("fs", ("sp", "tp"), None),
        check_vma=False,
    )
```

```python
import jax
import jax.numpy as jnp
from jax import lax
from jax.experimental import pallas as pl
from jax.experimental.pallas import tpu as pltpu
from jax.sharding import PartitionSpec as P

epsilon = 1e-06
log2e = 1.4426950408889634
bf16, f32 = jnp.bfloat16, jnp.float32
vmem = pl.BlockSpec(memory_space=pltpu.VMEM)
smem = pl.BlockSpec(memory_space=pltpu.SMEM)
rows_by_rows = (((1,), (1,)), ((), ()))


def struct(shape, kind):
    return jax.ShapeDtypeStruct(shape, kind)


def dot(a, b):
    return jnp.dot(a, b, preferred_element_type=f32)


def copies_of(x, axis):
    return jnp.broadcast_to(x, (lax.axis_size(axis), *x.shape))


def exchanged(x, axis):
    return lax.all_to_all(x, axis, split_axis=0, concat_axis=0, tiled=True)


def from_everyone(x, axis):
    return exchanged(copies_of(x, axis), axis)


def side_by_side_kernel(*refs):
    at = 0
    for ref in refs[:-1]:
        refs[-1][:, at : at + ref.shape[1]] = ref[...]
        at += ref.shape[1]


def side_by_side(*arrays):
    columns = sum(a.shape[1] for a in arrays)
    return pl.pallas_call(
        side_by_side_kernel,
        out_shape=struct((arrays[0].shape[0], columns), arrays[0].dtype),
        in_specs=[vmem] * len(arrays),
        out_specs=vmem,
        name="side_by_side",
    )(*arrays)


def put_rows_in_order(tiles_ref, first, count, out_ref, piece):
    fs, rows, _ = tiles_ref.shape
    for z in range(rows // piece):
        for y in range(fs):
            at = (z * fs + y) * piece
            out_ref[at : at + piece, :] = tiles_ref[
                y, z * piece : (z + 1) * piece, first : first + count
            ]


def start_rows(w_ref, first, count, out_ref, sems):
    copies = []
    for y in range(w_ref.shape[0]):
        copies.append(
            pltpu.make_async_copy(
                w_ref.at[y, :, :, pl.ds(first, count)], out_ref.at[:, y], sems.at[y]
            )
        )
        copies[-1].start()
    return copies


def wait_rows(copies, out_ref):
    for copy in copies:
        copy.wait()
    sp, fs, piece, n = out_ref.shape
    return out_ref[...].reshape(sp * fs * piece, n)


def twice(gain_ref):
    return jnp.concatenate([gain_ref[...], gain_ref[...]], axis=1)


def halves_normed(x, gain):
    half = x.shape[1] // 2
    low = lax.broadcasted_iota(jnp.int32, x.shape, 1) < half
    squares = x * x
    zero = jnp.zeros_like(squares)
    one = jnp.sum(jnp.where(low, squares, zero), axis=1, keepdims=True) / half
    two = jnp.sum(jnp.where(low, zero, squares), axis=1, keepdims=True) / half
    return x * jnp.where(low, lax.rsqrt(one + epsilon), lax.rsqrt(two + epsilon)) * gain


def key_value_kernel(x_ref, gain_ref, w_ref, key_gain_ref, normed_ref, kv_ref, rows_ref, piece):
    blocks, tok, feat = x_ref.shape
    put_rows_in_order(w_ref, 0, w_ref.shape[2], rows_ref, piece)
    squares = jnp.zeros((tok, feat), f32)
    for b in range(blocks):
        x = x_ref[b].astype(f32)
        squares = squares + x * x
    mean = jnp.sum(squares, axis=1, keepdims=True) / (blocks * feat)
    scale = lax.rsqrt(mean + epsilon)
    for b in range(blocks):
        normed_ref[:, b * feat : (b + 1) * feat] = (
            x_ref[b].astype(f32) * scale * gain_ref[:, b * feat : (b + 1) * feat]
        ).astype(bf16)
    both = dot(normed_ref[...], rows_ref[...])
    width = 2 * key_gain_ref.shape[1]
    kv_ref[:, :width] = halves_normed(both[:, :width], twice(key_gain_ref)).astype(bf16)
    kv_ref[:, width:] = both[:, width:].astype(bf16)


def query_kernel(
    x_ref, edge_ref, w_ref, gain_ref, all_taps_ref, me_ref, q_ref, filtered_ref,
    rows_ref, signal_ref, sems,
):
    tok, channels = filtered_ref.shape
    width = 2 * gain_ref.shape[1]
    weights = wait_rows(start_rows(w_ref, 0, w_ref.shape[3], rows_ref, sems), rows_ref)
    x = x_ref[...]
    q_ref[...] = halves_normed(dot(x, weights[:, :width]), twice(gain_ref)).astype(bf16)

    def signal_of(rows):
        both = dot(rows, weights[:, width:])
        return (both[:, :channels] * both[:, channels:]).astype(bf16).astype(f32)

    signal = signal_of(x)
    side = signal_of(edge_ref[...])
    signal_ref[8 : tok + 8, :] = signal
    signal_ref[7:8, :] = side[0:1]
    signal_ref[tok + 8 : tok + 9, :] = side[8:9]
    taps = all_taps_ref[:, pl.ds(pl.multiple_of(me_ref[0] * channels, channels), channels)]
    filtered_ref[...] = (
        taps[0:1, :] * signal_ref[7 : tok + 7, :]
        + taps[1:2, :] * signal
        + taps[2:3, :] * signal_ref[9 : tok + 9, :]
    )


def conv_kernel(x_ref, filtered_ref, w_ref, hidden_ref, rows_ref, sems):
    copies = start_rows(w_ref, 0, filtered_ref.shape[1], rows_ref, sems)
    post = dot(x_ref[...], wait_rows(copies, rows_ref)).astype(bf16).astype(f32)
    hidden_ref[...] = (post * filtered_ref[...]).astype(bf16)


def attention_kernel(
    q_ref, kv_ref, lam_ref, gain_ref, conv_ref, out_w_ref, me_ref, mine_ref, theirs_ref,
    acc_ref, both_ref, one_ref, two_ref, all_ref, conv_in_ref, rows_ref, out_ref,
    sems, w_sems, out_sems,
):
    tok, width = q_ref.shape
    half = width // 2
    vsize = gain_ref.shape[1]
    length = kv_ref.shape[0]
    block = one_ref.shape[0]
    steps = length // block
    me = me_ref[0]
    early = 3 * block

    def arrival(start, size, k):
        rows = pl.ds(start, size)
        return pltpu.make_async_copy(kv_ref.at[rows], all_ref.at[rows], sems.at[k])

    head, tail = arrival(0, early, 0), arrival(early, length - early, 1)
    head.start()
    tail.start()
    channels = conv_ref.shape[1]
    conv_copy = pltpu.make_async_copy(conv_ref, conv_in_ref, sems.at[2])
    conv_copy.start()
    copies = start_rows(out_w_ref, channels, rows_ref.shape[3], rows_ref, w_sems)
    q = q_ref[...].astype(f32) * (log2e * half ** (-0.5))
    high = q.astype(bf16)
    low = (q - high.astype(f32)).astype(bf16)
    lane = lax.broadcasted_iota(jnp.int32, q.shape, 1)
    zero = jnp.zeros_like(high)
    both = jnp.concatenate(
        [
            jnp.concatenate([jnp.where(mask, high, zero), jnp.where(mask, low, zero)], axis=1)
            for mask in (lane < half, lane >= half)
        ],
        axis=0,
    )
    both_ref[...] = jnp.transpose(both.astype(f32)).astype(bf16)
    acc_ref[...] = jnp.zeros_like(acc_ref)

    def rows_of(i):
        return pl.ds(pl.multiple_of(i * block, block), block)

    span = 256
    parts = [slice(n, n + span) for n in range(0, 2 * tok, span)]

    def scores_of(i, s_ref, part):
        key = all_ref[rows_of(i), :width]
        scores = dot(jnp.concatenate([key, key], axis=1), both_ref[:, part])
        s_ref[:, part] = scores
        return jnp.max(scores, axis=0, keepdims=True)

    ones = jnp.ones((block, acc_ref.shape[0] - vsize), bf16)

    def take(i, s_ref, part, top, peak):
        new_peak = jnp.maximum(peak, top)
        factor = jnp.exp2(peak - new_peak)
        expo = jnp.exp2(s_ref[:, part] - new_peak)
        acc_ref[:, part] = acc_ref[:, part] * factor + lax.dot_general(
            jnp.concatenate([all_ref[rows_of(i), width:], ones], axis=1), expo.astype(bf16),
            (((0,), (0,)), ((), ())), preferred_element_type=f32,
        )
        return new_peak

    def stage(i, state, here, there):
        result = []
        for part, (top, peak) in zip(parts, state):
            next_top = scores_of(jnp.minimum(i + 1, steps - 1), there, part)
            result.append((next_top, take(i, here, part, top, peak)))
        return result

    def step(j, state):
        @pl.when(j == 1)
        def _():
            tail.wait()

        state = stage(2 * j, state, one_ref, two_ref)
        return stage(2 * j + 1, state, two_ref, one_ref)

    head.wait()
    lowest = jnp.full((1, span), -1e30, f32)
    state = [(scores_of(0, one_ref, part), lowest) for part in parts]
    lax.fori_loop(0, steps // 2, step, state)
    mapped = acc_ref[:vsize] / acc_ref[vsize : vsize + 1]
    out = mapped[:, :tok] - lam_ref[me] * mapped[:, tok:]
    scaled = out * lax.rsqrt(jnp.mean(out * out, axis=0, keepdims=True) + epsilon)
    hidden = (jnp.transpose(scaled) * gain_ref[...]).astype(bf16)
    weights = wait_rows(copies, rows_ref)
    conv_copy.wait()
    rows = jnp.concatenate([conv_in_ref[...], hidden], axis=1)
    chips, count, _ = mine_ref.shape
    first_core = (me & 1) == 0
    leaving = []
    for k, ref in enumerate((theirs_ref, mine_ref)):
        chosen = []
        for chip in range(chips):
            one = rows[2 * chip * count : (2 * chip + 1) * count]
            two = rows[(2 * chip + 1) * count : (2 * chip + 2) * count]
            chosen.append(jnp.where(first_core == (k == 1), one, two))
        part = lax.dot_general(
            jnp.concatenate(chosen, axis=0), weights, rows_by_rows, preferred_element_type=f32
        ).astype(bf16)
        for chip in range(chips):
            out_ref[k, chip] = part[chip * count : (chip + 1) * count]
        leaving.append(pltpu.make_async_copy(out_ref.at[k], ref, out_sems.at[k]))
        leaving[-1].start()
    for copy in leaving:
        copy.wait()


def per_device(
    inputs,
    norm_gain,
    query_weight,
    key_weight,
    value_weight,
    query_gain,
    key_gain,
    mix_lambda,
    head_gain,
    post_gate_weight,
    pre_gate_weight,
    inner_weight,
    conv_taps,
    attn_out_weight,
    conv_out_weight,
):
    tokens = inputs[0]
    tok, feat = tokens.shape
    sp, tp = lax.axis_size("sp"), lax.axis_size("tp")
    total_feat = tp * feat
    width = key_weight.shape[1]
    vsize = head_gain.shape[0]
    channels = post_gate_weight.shape[1]
    piece = key_weight.shape[0]
    out_rows = tok // tp
    chips = tp // 2
    me = lax.axis_index("tp").astype(jnp.int32).reshape(1)
    key_gain, query_gain = key_gain.reshape(1, -1), query_gain.reshape(1, -1)
    in_hbm = pl.BlockSpec(memory_space=pl.ANY)

    def by_rows(tiles):
        return tiles.reshape(tiles.shape[0], sp, piece, tiles.shape[2])

    def ordered(columns):
        return pltpu.VMEM((sp, total_feat // (sp * piece), piece, columns), bf16)

    def sems(count):
        return pltpu.SemaphoreType.DMA((count,))

    fs = lax.axis_size("fs")

    whole = lax.all_gather(tokens, "tp", axis=0, tiled=False)
    first = side_by_side(
        key_weight, value_weight, query_weight, pre_gate_weight, inner_weight
    )
    first = lax.all_gather(first, "sp", axis=0, tiled=True)
    kv_weight = from_everyone(first[:, : width + vsize], "fs")
    normed, kv = pl.pallas_call(
        lambda *refs: key_value_kernel(*refs, piece=piece),
        out_shape=(struct((tok, total_feat), bf16), struct((tok, width + vsize), bf16)),
        in_specs=[vmem] * 4,
        out_specs=(vmem, vmem),
        scratch_shapes=[pltpu.VMEM((total_feat, width + vsize), bf16)],
        name="key_value",
    )(whole, norm_gain.reshape(1, total_feat), kv_weight, key_gain)
    kv_all = lax.all_gather(kv, "sp", axis=0, tiled=True)

    up = [(i, i + 1) for i in range(sp - 1)]
    before = lax.ppermute(normed[tok - 8 :], "sp", up)
    after = lax.ppermute(normed[:8], "sp", [(j, i) for i, j in up])
    edge = jnp.concatenate([before[7:], before[:7], after], axis=0)

    one, _ = lax.optimization_barrier((copies_of(first[:, width + vsize :], "fs"), kv_weight))
    one = exchanged(one, "fs")
    second = side_by_side(post_gate_weight, conv_out_weight, attn_out_weight)
    second, _ = lax.optimization_barrier((second, kv))
    second = lax.all_gather(second, "sp", axis=0, tiled=True)
    query, filtered = pl.pallas_call(
        query_kernel,
        out_shape=(struct((tok, width), bf16), struct((tok, channels), f32)),
        in_specs=[vmem, vmem, in_hbm, vmem, vmem, smem],
        out_specs=(vmem, vmem),
        scratch_shapes=[
            ordered(width + 2 * channels),
            pltpu.VMEM((tok + 16, channels), f32),
            sems(fs),
        ],
        name="query",
    )(normed, edge, by_rows(one), query_gain, conv_taps, me)

    two = by_rows(from_everyone(second, "fs"))
    conv_hidden = pl.pallas_call(
        conv_kernel,
        out_shape=struct((tok, channels), bf16),
        in_specs=[vmem, vmem, in_hbm],
        out_specs=vmem,
        scratch_shapes=[ordered(channels), sems(fs)],
        name="conv",
    )(normed, filtered, two)

    mine, theirs = pl.pallas_call(
        attention_kernel,
        out_shape=(struct((chips, out_rows, total_feat), bf16),) * 2,
        in_specs=[vmem, in_hbm, smem, vmem, in_hbm, in_hbm, smem],
        out_specs=(in_hbm, in_hbm),
        scratch_shapes=[
            pltpu.VMEM((vsize + 8, 2 * tok), f32),
            pltpu.VMEM((2 * width, 2 * tok), bf16),
        ]
        + [pltpu.VMEM((512, 2 * tok), f32)] * 2
        + [pltpu.VMEM(kv_all.shape, bf16), pltpu.VMEM((tok, channels), bf16)]
        + [ordered(channels + vsize), pltpu.VMEM((2, chips, out_rows, total_feat), bf16)]
        + [sems(3), sems(fs), sems(2)],
        cost_estimate=pl.CostEstimate(
            flops=8 * tok * kv_all.shape[0] * vsize, bytes_accessed=kv_all.size * 2, transcendentals=0
        ),
        name="attention",
    )(query, kv_all, mix_lambda, head_gain.reshape(1, vsize), conv_hidden, two, me)
    theirs = lax.ppermute(theirs, "tp", [(i, i ^ 1) for i in range(tp)])
    part = (mine.astype(f32) + theirs.astype(f32)).astype(bf16)
    same_core = [list(range(c, tp, 2)) for c in range(2)]
    arrived = lax.all_to_all(
        part, "tp", split_axis=0, concat_axis=0, tiled=True, axis_index_groups=same_core
    )
    return jnp.sum(arrived.astype(f32), axis=0).astype(bf16)[None]


def solution(mesh):
    weight = P(("sp", "fs"), "tp")
    placed = (P("fs", "sp", "tp"), P(), weight, weight, weight, P(), P(), P(), P())
    placed = placed + (weight, weight, weight, P(), weight, weight)
    return jax.shard_map(
        per_device,
        mesh=mesh,
        in_specs=placed,
        out_specs=P("fs", ("sp", "tp"), None),
        check_vma=False,
    )
```
